256 devices in a mesh: ep: 16 (over y, x), tp: 16 (over z, core).
Axes of the slice: x: 4, y: 4, z: 8, core: 2. Of those that a mesh axis runs over, the one named last changes fastest.
Arguments:
- tokens: bfloat16 [256, 2048], P('ep'), may hold values from -6 to 6
- norm_gain: float32 [2048], replicated, may hold values from 0.1 to 1.9
- w_query: bfloat16 [2048, 2048], P('ep', 'tp'), may hold values from -0.125 to 0.125
- w_key: bfloat16 [2048, 2048], P('ep', 'tp'), may hold values from -0.125 to 0.125
- w_value: bfloat16 [2048, 2048], P('ep', 'tp'), may hold values from -0.125 to 0.125
- w_forget: bfloat16 [2048, 16], replicated, may hold values from -0.125 to 0.125
- forget_bias: float32 [16], replicated, may hold values from -1 to 2
- query_gain: float32 [128], replicated, may hold values from 0.1 to 1.9
- key_gain: float32 [128], replicated, may hold values from 0.1 to 1.9
- cache_keys: bfloat16 [256, 16, 1024, 128], P('ep', 'tp'), may hold values from -400 to 400
- cache_values: bfloat16 [256, 16, 1024, 128], P('ep', 'tp'), may hold values from -6 to 6
- cache_gates: float32 [256, 16, 1024], P('ep', 'tp'), may hold values from -144 to 0, as said below
- lengths: int32 [256], P('ep'), may hold values from 1 to 1024, 131072 in all
- w_output: bfloat16 [2048, 2048], P('tp'), may hold values from -0.375 to 0.375
- ffn_gain: float32 [2048], replicated, may hold values from 0.1 to 1.9
- routes: int32 [256, 2], P('ep'), may hold values from 0 to 31, all different within a row; in each aligned block of 16 rows (0 to 15, 16 to 31, ...) at most 2 rows name the same one
- route_weights: float32 [256, 2], P('ep'), may hold values from 0.2 to 1
- w_gate: bfloat16 [32, 2048, 2048], P('ep', None, 'tp'), may hold values from -0.125 to 0.125
- w_up: bfloat16 [32, 2048, 2048], P('ep', None, 'tp'), may hold values from -0.125 to 0.125
- w_down: bfloat16 [32, 2048, 2048], P('ep', 'tp'), may hold values from -0.125 to 0.125
Outputs:
- result: bfloat16 [256, 2048], P('ep', 'tp')
The draws below stay inside these ranges and needn't reach their ends.
Inputs may be any that keep to these rules, and one draw needn't show every extreme that they name: `routes`: within the rows of one index of ep (16 sequences) no expert is named by more than 2 rows, a bound that some block reaches; each row names 2 different experts. `lengths`: one sequence has exactly 1024 cached positions. `cache_gates`: along positions, the values of each sequence and head never rise.
All inputs are finite; a program needn't handle non-finite values. No bound on the sum of `lengths` on one device may be relied on, other than what follows from the above.
Results may differ from the reference program's by a relative error of at most 0.012.
The reference program's roundings to bfloat16 on the way count: a program that leaves them out, or rounds other values in their place, can miss the bound.
Values may be sent and summed in bfloat16 or wider, within the bound.
A program may use at most 64 MiB of HBM per device.

```python
import math
import jax
import jax.numpy as jnp
import numpy as np
from jax import lax

D = 2048
HEADS = 16
HD = 128
FF = 2048
TOP_K = 2
SEQ_GRP = 16
CACHE_POSITIONS = 1024
TOKENS = 256
EXPERTS = 32
CAP = 2


def draw_cache_keys(key, part):
    array_extent = (TOKENS, HEADS, CACHE_POSITIONS, HD)
    base = jax.random.normal(jax.random.fold_in(key, 3), array_extent, jnp.float32)
    return jnp.clip(base, -6.0, 6.0).astype(jnp.bfloat16)


def draw_cache_gates(key, part):
    array_extent = (TOKENS, HEADS, CACHE_POSITIONS)
    head_random_key, sequence_random_key, coarse_random_key, spike_random_key, discard_random_key = jax.random.split(jax.random.fold_in(key, 7), 5)
    slow_share = 0.5
    sluggish_heads = jax.random.uniform(head_random_key, (HEADS,)) < slow_share
    rate = jnp.where(sluggish_heads, 0.5 / CACHE_POSITIONS, 1.0 / 40.0)[None, :, None]
    seq_factor = jnp.exp(jax.random.uniform(sequence_random_key, (TOKENS, 1, 1), jnp.float32, -0.7, 0.7))
    rough = jnp.exp(jax.random.uniform(coarse_random_key, array_extent, jnp.float32, -0.7, 0.7))
    decode_steps = -rate * seq_factor * rough
    spike_events = (jax.random.uniform(spike_random_key, array_extent) < 2.0 / CACHE_POSITIONS) & sluggish_heads[None, :, None]
    discard_events = jnp.log(jax.random.uniform(discard_random_key, array_extent, jnp.float32, 0.5, 0.8))
    decode_steps = decode_steps + jnp.where(spike_events, discard_events, 0.0)
    return jnp.cumsum(decode_steps, axis=2)


def block_scale(key, dims, cuts, smallest, high):
    loudness, own = 1.0, jax.random.fold_in(key, 6)
    for dim, shards_of in cuts:
        heights = jnp.exp(jax.random.uniform(jax.random.fold_in(own, dim), (shards_of,), jnp.float32, smallest / len(cuts), high / len(cuts)))
        loudness = loudness * jnp.repeat(heights, dims[dim] // shards_of).reshape([-1 if axis == dim else 1 for axis in range(len(dims))])
    return loudness


def profile(count, total, limit, skew):
    loads = [(1 << 20) // math.isqrt(rank ** skew) + 1 for rank in range(2, count + 1)]
    surplus, holding = total - limit - (count - 1), [1] * (count - 1)
    while surplus > 0:
        movable = [i for i in range(count - 1) if holding[i] < limit]
        mass, budget = sum([loads[i] for i in movable]), surplus
        for i in movable:
            more = min(limit - holding[i], max(1, budget * loads[i] // mass), surplus)
            holding[i] = holding[i] + more
            surplus = surplus - more
    return np.array([limit] + holding)


def ragged(key, number_of, total, most, skew):
    if number_of == 2:
        one = jax.random.randint(key, (), max(1, total - most), min(most, total - 1) + 1)
        return jnp.stack([one, total - one])
    sizes = jnp.asarray(profile(number_of, total, most, skew), jnp.int32)
    couples = (number_of - 1) // 2
    giver, taker = sizes[1:1 + 2 * couples:2], sizes[2:2 + 2 * couples:2]
    margin = jnp.minimum(giver - 1, most - taker)
    passed = jax.random.randint(jax.random.fold_in(key, 1), (couples,), 0, 1 << 20) % (margin + 1)
    sizes = sizes.at[1:1 + 2 * couples:2].set(giver - passed).at[2:2 + 2 * couples:2].set(taker + passed)
    return sizes[jax.random.permutation(jax.random.fold_in(key, 2), number_of)]


def routed_block(key, own, number, rows, amount, top, most, lean):
    order = jax.random.permutation(key, amount)
    heavy_load, common = shares(amount, rows * top, most, lean, True), shares(amount, rows * top, most, lean, False)
    places = jnp.arange(amount)

    def named(tallies, turn):
        used = int((tallies > 0).sum())
        fixed = max(1, used // 4)
        passed = fixed + (places - fixed + turn * (used - fixed)) % max(1, amount - fixed)
        return jnp.zeros((amount,), jnp.int32).at[order[jnp.where(places < fixed, places, passed)]].set(jnp.asarray(tallies, jnp.int32))

    tallies = jnp.where(number % 4 == 0, named(heavy_load, number // 4), named(common, number - number // 4 - 1))
    mixed = jax.random.permutation(jax.random.fold_in(own, 3), amount)
    donor, taker = mixed[0:amount // 2 * 2:2], mixed[1:amount // 2 * 2:2]
    margin = jnp.minimum(tallies[donor] - 1, most - tallies[taker]) // 2
    margin = jnp.where((donor == order[0]) | (taker == order[0]) | (tallies[taker] == 0), 0, jnp.maximum(margin, 0))
    passed = jax.random.randint(jax.random.fold_in(own, 4), (amount // 2,), 0, 1 << 20) % (margin + 1)
    tallies = tallies.at[donor].add(-passed).at[taker].add(passed)
    members = jnp.searchsorted(jnp.cumsum(tallies), jnp.arange(rows * top), side="right").astype(jnp.int32)
    table = members.reshape(top, rows).T
    table = table[jax.random.permutation(jax.random.fold_in(own, 1), rows)]
    turn = jax.random.randint(jax.random.fold_in(own, 2), (rows, 1), 0, top)
    return jnp.take_along_axis(table, (jnp.arange(top)[None, :] + turn) % top, axis=1)


def shares(amount, total, limit, slope, full):
    weights = [(1 << 20) // math.isqrt(standing ** slope) + 1 for standing in range(1, amount + 1)]
    largest = limit if full else min(limit, max(-(-total // amount), total * weights[0] // sum(weights)))
    least = 1 if total - largest >= amount - 1 else 0
    counts, rest = [largest] + [least] * (amount - 1), total - largest - least * (amount - 1)
    while rest > 0:
        candidates = [i for i in range(1, amount) if counts[i] < largest] or [i for i in range(1, amount) if counts[i] < limit]
        pool, remaining = sum([weights[i] for i in candidates]), rest
        for i in candidates:
            addition = min(limit - counts[i], max(1, remaining * weights[i] // pool), rest)
            counts[i] = counts[i] + addition
            rest = rest - addition
    return np.array(counts)


def bell_draw(key, dims, spread, limit, pieces=(), held_as=jnp.bfloat16):
    loudness = block_scale(key, dims, pieces, -0.22, 0.18) if pieces else 1.0
    values = jax.random.normal(key, dims, jnp.float32) * spread * loudness
    return jnp.minimum(jnp.maximum(values, -limit), limit).astype(held_as)


def setup_inputs(seed: int = 0) -> dict:
    keys = jax.random.split(jax.random.key(seed), 21)
    tokens = bell_draw(keys[0], (TOKENS, D), 1.0, 6.0, ((0, 16),))
    norm_gain = jnp.clip(1.0 + 0.18 * jax.random.normal(keys[1], (D,), jnp.float32), 0.1, 1.9)
    w_query = bell_draw(keys[2], (D, HEADS * HD), D ** -0.5, 0.125, ((0, 16), (1, 16)))
    w_key = bell_draw(keys[3], (D, HEADS * HD), D ** -0.5, 0.125, ((0, 16), (1, 16)))
    w_value = bell_draw(keys[4], (D, HEADS * HD), D ** -0.5, 0.125, ((0, 16), (1, 16)))
    w_forget = bell_draw(keys[5], (D, HEADS), D ** -0.5, 0.125)
    forget_bias = jnp.clip(jax.random.uniform(keys[6], (HEADS,), jnp.float32, -1.0, 2.0), -1.0, 2.0)
    query_gain = jnp.clip(1.0 + 0.18 * jax.random.normal(keys[7], (HD,), jnp.float32), 0.1, 1.9)
    key_gain = jnp.clip(1.0 + 0.18 * jax.random.normal(keys[8], (HD,), jnp.float32), 0.1, 1.9)
    cache_keys = draw_cache_keys(jax.random.fold_in(keys[20], 71), 0)
    cache_values = bell_draw(keys[10], (TOKENS, HEADS, CACHE_POSITIONS, HD), 1.0, 6.0, ((0, 16), (1, 16)))
    cache_gates = draw_cache_gates(jax.random.fold_in(keys[20], 71), 0)
    lengths = ragged(keys[12], TOKENS, TOKENS * CACHE_POSITIONS // 2, CACHE_POSITIONS, 2).astype(jnp.int32)
    w_output = bell_draw(keys[13], (HEADS * HD, D), (HEADS * HD // 8) ** -0.5, 0.375, ((0, 16),))
    ffn_gain = jnp.clip(1.0 + 0.18 * jax.random.normal(keys[14], (D,), jnp.float32), 0.1, 1.9)
    routes_keys = jax.random.split(jax.random.fold_in(keys[15], 1), TOKENS // SEQ_GRP)
    routes_turns = jax.random.permutation(jax.random.fold_in(keys[15], 3), TOKENS // SEQ_GRP)
    routes = jax.vmap(lambda own, number: routed_block(jax.random.fold_in(keys[15], 2), own, number, SEQ_GRP, EXPERTS, TOP_K, CAP, 2))(routes_keys, routes_turns).reshape((TOKENS, TOP_K))
    route_weights = jnp.clip(0.2 + 0.8 * jax.random.uniform(keys[16], (TOKENS, TOP_K), jnp.float32) ** block_scale(keys[16], (TOKENS, TOP_K), ((0, 16),), -0.2, 0.2), 0.2, 1.0)
    w_gate = bell_draw(keys[17], (EXPERTS, D, FF), D ** -0.5, 0.125, ((0, 16), (2, 16)))
    w_up = bell_draw(keys[18], (EXPERTS, D, FF), D ** -0.5, 0.125, ((0, 16), (2, 16)))
    w_down = bell_draw(keys[19], (EXPERTS, FF, D), FF ** -0.5, 0.125, ((0, 16), (1, 16)))
    return dict(tokens=tokens, norm_gain=norm_gain, w_query=w_query, w_key=w_key, w_value=w_value, w_forget=w_forget, forget_bias=forget_bias, query_gain=query_gain, key_gain=key_gain, cache_keys=cache_keys, cache_values=cache_values, cache_gates=cache_gates, lengths=lengths, w_output=w_output, ffn_gain=ffn_gain, routes=routes, route_weights=route_weights, w_gate=w_gate, w_up=w_up, w_down=w_down)


epsilon = 1e-06

def norm_rows(values, gain_row):
    widened = values.astype(jnp.float32)
    scaled = widened * lax.rsqrt(lax.optimization_barrier(jnp.mean(widened * widened, axis=-1, keepdims=True)) + epsilon)
    return scaled * gain_row.astype(jnp.float32)

def reference(tokens, norm_gain, w_query, w_key, w_value, w_forget, forget_bias, query_gain, key_gain, cache_keys, cache_values, cache_gates, lengths, w_output, ffn_gain, routes, route_weights, w_gate, w_up, w_down):
    normed = norm_rows(tokens, norm_gain).astype(jnp.bfloat16)
    query_raw = jnp.dot(normed, w_query, preferred_element_type=jnp.float32).reshape(TOKENS, HEADS, HD)
    key_raw = jnp.dot(normed, w_key, preferred_element_type=jnp.float32).reshape(TOKENS, HEADS, HD)
    value_raw = jnp.dot(normed, w_value, preferred_element_type=jnp.float32).reshape(TOKENS, HEADS, HD)
    queries = norm_rows(query_raw, query_gain).astype(jnp.bfloat16)
    keys_new = norm_rows(key_raw, key_gain).astype(jnp.bfloat16)
    values_new = value_raw.astype(jnp.bfloat16)
    forget = jax.nn.log_sigmoid(jnp.dot(normed, w_forget, preferred_element_type=jnp.float32) + forget_bias)
    score_scale = HD ** (-0.5)
    positions = jnp.arange(CACHE_POSITIONS, dtype=jnp.int32)

    def attend_one(inputs):
        query_now, key_now, value_now, key_rows, value_rows, gate_rows, length, forget_now = inputs
        live_mask = positions < length
        last_gate = lax.optimization_barrier(jnp.sum(jnp.where(positions[None, :] == length - 1, gate_rows, 0.0), axis=-1))
        scores = jnp.einsum('hd,hld->hl', query_now.astype(jnp.float32), key_rows.astype(jnp.float32)) * score_scale
        scores = scores + (last_gate[:, None] - gate_rows) + forget_now[:, None]
        scores = jnp.where(live_mask[None, :], scores, -1e+30)
        own_score = lax.optimization_barrier(jnp.sum(query_now.astype(jnp.float32) * key_now.astype(jnp.float32), axis=-1)) * score_scale
        row_peak = jnp.maximum(lax.optimization_barrier(jnp.max(scores, axis=-1)), own_score)
        weights = jnp.exp(scores - row_peak[:, None])
        own_weight = jnp.exp(own_score - row_peak)
        denominator = lax.optimization_barrier(jnp.sum(weights, axis=-1)) + own_weight
        probabilities = (weights / denominator[:, None]).astype(jnp.bfloat16)
        own_prob = (own_weight / denominator).astype(jnp.bfloat16)
        attended_row = jnp.einsum('hl,hld->hd', probabilities.astype(jnp.float32), value_rows.astype(jnp.float32))
        attended_row = attended_row + own_prob.astype(jnp.float32)[:, None] * value_now.astype(jnp.float32)
        return attended_row.astype(jnp.bfloat16).reshape(HEADS * HD)
    attended = lax.map(attend_one, (queries, keys_new, values_new, cache_keys, cache_values, cache_gates, lengths, forget))
    attention = jnp.dot(attended, w_output, preferred_element_type=jnp.float32)
    mixed_rows = (tokens.astype(jnp.float32) + attention).astype(jnp.bfloat16)
    normed_ffn = norm_rows(mixed_rows, ffn_gain).astype(jnp.bfloat16)
    fractions = route_weights / lax.optimization_barrier(jnp.sum(route_weights, axis=-1, keepdims=True))
    item_rows = jnp.repeat(normed_ffn, TOP_K, axis=0)

    def expert_one(inputs):
        token_row, expert = inputs
        gate_part = jnp.dot(token_row[None, :], w_gate[expert], preferred_element_type=jnp.float32)
        upper_part = jnp.dot(token_row[None, :], w_up[expert], preferred_element_type=jnp.float32)
        hidden = (jax.nn.silu(gate_part) * upper_part).astype(jnp.bfloat16)
        return jnp.dot(hidden, w_down[expert], preferred_element_type=jnp.float32)[0].astype(jnp.bfloat16)
    expert_out = lax.map(expert_one, (item_rows, routes.reshape(TOKENS * TOP_K)))
    combined = lax.optimization_barrier(jnp.sum(fractions[:, :, None] * expert_out.reshape(TOKENS, TOP_K, D).astype(jnp.float32), axis=1))
    return (mixed_rows.astype(jnp.float32) + combined).astype(jnp.bfloat16)
```

```python
import functools

import jax
import jax.numpy as jnp
from jax import lax
from jax.experimental import pallas as pl
from jax.experimental.pallas import tpu as pltpu
from jax.sharding import PartitionSpec as P

MESH = pl.DeviceIdType.MESH
F32 = jnp.float32
BF16 = jnp.bfloat16
EPS = 1e-06
CAP = 2
LANES = 128

CH_X, CH_Q, CH_KV, CH_O, CH_M, CH_D, CH_R, CH_F = range(8)


def norm(v, gain):
    return v * lax.rsqrt(jnp.mean(v * v, axis=-1, keepdims=True) + EPS) * gain


def dot(a, b):
    return jnp.dot(a, b, preferred_element_type=F32)


def dot_t(a, b):
    return lax.dot_general(a, b, (((1,), (1,)), ((), ())), preferred_element_type=F32)


def swap_halves(a, b):
    low = lax.broadcasted_iota(jnp.int32, a.shape, 1) < 4
    a_turned, b_turned = pltpu.roll(a, 4, 1), pltpu.roll(b, 4, 1)
    return jnp.where(low, a, b_turned), jnp.where(low, a_turned, b)


def kernel(ep, tp, *refs):
    names = (
        "tokens", "norm_gain", "wq", "wk", "wv", "wf", "f_bias", "q_gain", "k_gain", "keys",
        "values", "gates", "lengths", "wo", "ffn_gain", "routes", "r_weights", "wg", "wu", "wd",
    )
    hbm = dict(zip(names, refs))
    out_ref = refs[len(names)]
    (
        tok_v, ng_v, wqkv_v, wf_v, fb_v, qg_v, kg_v, k_v, v_v, g_v, len_v,
        wo_v, fg_v, rt_v, rw_v, wgu_v, wd_v,
        xs, xr, qs, qr, kvs, kvr, os_, or_, ms, mr, ds_, dr, rs, rr, fs, fr,
        big, xe,
        hsem, ssem, rsem,
    ) = refs[len(names) + 1 :]

    me_e, me_t = lax.axis_index("ep"), lax.axis_index("tp")
    rows, width = tok_v.shape
    span, hd = k_v.shape[1], k_v.shape[2]
    n_blocks = width // LANES
    depth = xs.shape[2]
    slots = 2 * CAP
    n_slots = ep * slots

    fetches = {}

    def fetch(name, pairs):
        fetches[name] = []
        for src, dst in pairs:
            at = sum(len(f) for f in fetches.values())
            copy = pltpu.make_async_copy(src, dst, hsem.at[at])
            copy.start()
            fetches[name].append(copy)

    def need(*which):
        for name in which:
            for copy in fetches[name]:
                copy.wait()

    fetch("tok", [(hbm["tokens"], tok_v), (hbm["norm_gain"], ng_v)])
    fetch(
        "wqkv",
        [(hbm[w], wqkv_v.at[:, pl.ds(i * hd, hd)]) for i, w in enumerate(("wq", "wk", "wv"))],
    )
    fetch(
        "small",
        [
            (hbm["wf"], wf_v), (hbm["f_bias"], fb_v), (hbm["q_gain"], qg_v),
            (hbm["k_gain"], kg_v), (hbm["gates"], g_v), (hbm["lengths"], len_v),
            (hbm["ffn_gain"], fg_v), (hbm["routes"], rt_v), (hbm["r_weights"], rw_v),
        ],
    )
    quarter = rows // 4
    fetch(
        "k",
        [(hbm["keys"].at[pl.ds(i * quarter, quarter), 0], k_v.at[pl.ds(i * quarter, quarter)]) for i in range(4)],
    )
    fetch(
        "v",
        [(hbm["values"].at[pl.ds(i * quarter, quarter), 0], v_v.at[pl.ds(i * quarter, quarter)]) for i in range(4)],
    )
    fetch("wo", [(hbm["wo"], wo_v)])
    hidden = hbm["wg"].shape[2]
    fetch(
        "wgu",
        [
            (hbm[w].at[x], wgu_v.at[:, pl.ds((2 * x + i) * hidden, hidden)])
            for x in range(2)
            for i, w in enumerate(("wg", "wu"))
        ],
    )
    fetch("wd", [(hbm["wd"].at[x], wd_v.at[pl.ds(x * hidden, hidden)]) for x in range(2)])

    barrier = pltpu.get_barrier_semaphore()

    def greet(axis, me, n):
        def body(i, carry):
            pl.semaphore_signal(
                barrier, inc=1, device_id={axis: lax.rem(me + i, n)}, device_id_type=MESH
            )
            return carry

        lax.fori_loop(1, n, body, 0)

    greet("ep", me_e, ep)
    greet("tp", me_t, tp)

    def send(axis, me, n, channel, src, dst):
        def body(i, carry):
            peer = lax.rem(me + i, n)
            pltpu.make_async_remote_copy(
                src_ref=src(peer),
                dst_ref=dst.at[me],
                send_sem=ssem.at[channel],
                recv_sem=rsem.at[channel],
                device_id={axis: peer},
                device_id_type=MESH,
            ).start()
            return carry

        lax.fori_loop(1, n, body, 0)

    def wait_all(n, sem, buf):
        part = buf.at[pl.ds(0, n - 1)]
        pltpu.make_async_copy(part, part, sem).wait()

    need("tok")
    normed = norm(tok_v[...].astype(F32), ng_v[...]).astype(BF16)
    for j in range(ep):
        xs[j] = normed[:, j * depth : (j + 1) * depth]
    xr[pl.ds(me_e, 1)] = xs[pl.ds(me_e, 1)]
    pl.semaphore_wait(barrier, ep + tp - 2)
    send("ep", me_e, ep, CH_X, lambda j: xs.at[j], xr)

    need("small")
    row = lax.broadcasted_iota(jnp.int32, (rows, 1), 0)
    diagonal = lax.broadcasted_iota(jnp.int32, (rows, rows), 0) == lax.broadcasted_iota(
        jnp.int32, (rows, rows), 1
    )

    def as_column(line):
        return jnp.sum(jnp.where(diagonal, line, jnp.zeros_like(line)), axis=1, keepdims=True)

    biased = dot_t(normed, wf_v[...]) + fb_v[...]
    own_head = lax.broadcasted_iota(jnp.int32, biased.shape, 1) == me_t
    biased = jnp.sum(jnp.where(own_head, biased, 0.0), axis=1, keepdims=True)
    forget = jnp.minimum(biased, 0.0) - jnp.log1p(jnp.exp(-jnp.abs(biased)))

    lengths = as_column(len_v[...].astype(F32)).astype(jnp.int32)
    position = lax.broadcasted_iota(jnp.int32, (rows, span), 1)
    gates = jnp.zeros((rows, span), F32)
    for s in range(rows):
        gates = jnp.where(row == s, g_v[s], gates)
    last_gate = jnp.sum(jnp.where(position == lengths - 1, gates, 0.0), axis=1, keepdims=True)
    live = position < lengths

    first = rt_v[0:1, :]
    second = rt_v[1:2, :]
    slot_col = lax.broadcasted_iota(jnp.int32, (n_slots, rows), 0)
    expert_col, copy_col = lax.div(slot_col, CAP), lax.rem(slot_col, CAP)
    named = ((expert_col == first) | (expert_col == second)).astype(F32)
    before = (
        lax.broadcasted_iota(jnp.int32, (rows, rows), 0)
        < lax.broadcasted_iota(jnp.int32, (rows, rows), 1)
    ).astype(F32)
    earlier = dot(named.astype(BF16), before.astype(BF16))
    placing = jnp.where(earlier == copy_col.astype(F32), named, 0.0).astype(BF16)

    weight_sum = rw_v[0:1, :] + rw_v[1:2, :]
    share_a = as_column(rw_v[0:1, :] / weight_sum)
    share_b = as_column(rw_v[1:2, :] / weight_sum)
    route_a = as_column(first.astype(F32)).astype(jnp.int32)
    route_b = as_column(second.astype(F32)).astype(jnp.int32)
    slot_row = lax.broadcasted_iota(jnp.int32, (rows, n_slots), 1)
    expert_row, copy_row = lax.div(slot_row, CAP), lax.rem(slot_row, CAP)
    is_a, is_b = expert_row == route_a, expert_row == route_b
    after = (
        lax.broadcasted_iota(jnp.int32, (rows, rows), 1)
        < lax.broadcasted_iota(jnp.int32, (rows, rows), 0)
    ).astype(BF16)
    earlier_row = dot(after, (is_a | is_b).astype(F32).astype(BF16))
    combine = jnp.where(is_a, share_a, 0.0) + jnp.where(is_b, share_b, 0.0)
    combine = jnp.where(earlier_row == copy_row.astype(F32), combine, 0.0)
    combine_1 = combine.astype(BF16)
    rest = combine - combine_1.astype(F32)
    combine_2 = rest.astype(BF16)
    combine_3 = (rest - combine_2.astype(F32)).astype(BF16)
    combine_parts = jnp.concatenate([combine_1, combine_2, combine_3], axis=0)

    need("wqkv")
    wait_all(ep, rsem.at[CH_X], xr)
    part = dot(xr[...].reshape(ep * rows, depth), wqkv_v[...])
    qs[...] = part[:, :hd].reshape(ep, rows, hd)
    for j in range(ep):
        own = part[j * rows : (j + 1) * rows]
        kvs[j, 0:rows, :] = own[:, hd : 2 * hd].astype(BF16)
        kvs[j, rows : 2 * rows, :] = own[:, 2 * hd :].astype(BF16)
    qr[pl.ds(me_e, 1)] = qs[pl.ds(me_e, 1)]
    kvr[pl.ds(me_e, 1)] = kvs[pl.ds(me_e, 1)]
    send("ep", me_e, ep, CH_Q, lambda j: qs.at[j], qr)
    send("ep", me_e, ep, CH_KV, lambda j: kvs.at[j], kvr)
    need("k", "v")
    wait_all(ep, rsem.at[CH_Q], qr)
    queries = norm(jnp.sum(qr[...], axis=0), qg_v[...]).astype(BF16)

    score_scale = hd ** (-0.5)
    scores = jnp.zeros((rows, span), F32)
    for s in range(rows):
        scores = jnp.where(row == s, dot_t(queries, k_v[s]), scores)
    wait_all(ep, rsem.at[CH_KV], kvr)
    kv_raw = jnp.sum(kvr[...].astype(F32), axis=0)
    keys_new = norm(kv_raw[:rows], kg_v[...]).astype(BF16)
    values_new = kv_raw[rows:].astype(BF16)
    scores = scores * score_scale + (last_gate - gates) + forget
    scores = jnp.where(live, scores, -1e30)
    own_score = (
        jnp.sum(queries.astype(F32) * keys_new.astype(F32), axis=1, keepdims=True) * score_scale
    )
    peak = jnp.maximum(jnp.max(scores, axis=1, keepdims=True), own_score)
    weights = jnp.exp(scores - peak)
    own_weight = jnp.exp(own_score - peak)
    denominator = jnp.sum(weights, axis=1, keepdims=True) + own_weight
    probabilities = weights / denominator
    own_prob = (own_weight / denominator).astype(BF16).astype(F32)
    attended = own_prob * values_new.astype(F32)
    for s in range(rows):
        mine = jnp.where(row == s, probabilities, 0.0).astype(BF16)
        attended = attended + dot(mine, v_v[s])
    attended = attended.astype(BF16)

    need("wo")
    cols = or_.shape[2]
    partial = dot(attended, wo_v[...])
    for j in range(tp):
        os_[j] = partial[:, j * cols : (j + 1) * cols]
    or_[pl.ds(me_t, 1)] = os_[pl.ds(me_t, 1)]
    send("tp", me_t, tp, CH_O, lambda j: os_.at[j], or_)
    wait_all(tp, rsem.at[CH_O], or_)
    own_tokens = tok_v[:, pl.ds(pl.multiple_of(me_t * cols, cols), cols)].astype(F32)
    mixed = (own_tokens + jnp.sum(or_[...], axis=0)).astype(BF16)
    ms[...] = mixed
    mr[pl.ds(me_t, 1)] = mixed[None]
    send("tp", me_t, tp, CH_M, lambda j: ms, mr)
    need("wgu", "wd")
    wait_all(tp, rsem.at[CH_M], mr)

    squares = jnp.zeros((rows, 1), F32)
    for b in range(n_blocks):
        block = mr[b].astype(F32)
        squares = squares + jnp.sum(block * block, axis=1, keepdims=True)
    factor = lax.rsqrt(squares / width + EPS)
    for b in range(n_blocks):
        block = mr[b].astype(F32) * factor * fg_v[:, b * LANES : (b + 1) * LANES]
        big[b] = dot(placing, block.astype(BF16))

    def pack(dst):
        for pair in range(ep // 2):
            tile = big[:, pair * 8 : pair * 8 + 8, :].reshape(n_blocks // 2, 2, 8, LANES)
            even, odd = swap_halves(tile[:, 0], tile[:, 1])
            dst[2 * pair] = even.reshape(n_blocks * 4, LANES).astype(BF16)
            dst[2 * pair + 1] = odd.reshape(n_blocks * 4, LANES).astype(BF16)

    def unpack(src):
        for quad in range(ep // 4):
            halves = []
            for pair in (2 * quad, 2 * quad + 1):
                a = src[2 * pair].astype(F32).reshape(n_blocks // 2, 8, LANES)
                b = src[2 * pair + 1].astype(F32).reshape(n_blocks // 2, 8, LANES)
                halves.append(swap_halves(a, b))
            for odd in range(2):
                whole = jnp.concatenate([halves[0][odd], halves[1][odd]], axis=1).astype(BF16)
                for i in range(n_blocks // 2):
                    b = 2 * i + odd
                    xe[quad * 16 : quad * 16 + 16, b * LANES : (b + 1) * LANES] = whole[i]

    pack(ds_)
    dr[pl.ds(me_e, 1)] = ds_[pl.ds(me_e, 1)]
    send("ep", me_e, ep, CH_D, lambda j: ds_.at[j], dr)
    wait_all(ep, rsem.at[CH_D], dr)

    unpack(dr)
    both = dot(xe[...], wgu_v[...])
    kind = lax.div(lax.rem(lax.broadcasted_iota(jnp.int32, (n_slots, 1), 0), slots), CAP)
    parts = []
    for x in range(2):
        gate = both[:, 2 * x * hidden : (2 * x + 1) * hidden]
        upper = both[:, (2 * x + 1) * hidden : (2 * x + 2) * hidden]
        parts.append(jnp.where(kind == x, gate * jax.nn.sigmoid(gate) * upper, 0.0))
    hidden_rows = jnp.concatenate(parts, axis=1).astype(BF16)
    expert_rows = dot(hidden_rows, wd_v[...])
    for b in range(n_blocks):
        big[b] = expert_rows[:, b * LANES : (b + 1) * LANES]
    pack(rs)
    rr[pl.ds(me_e, 1)] = rs[pl.ds(me_e, 1)]
    send("ep", me_e, ep, CH_R, lambda j: rs.at[j], rr)
    wait_all(ep, rsem.at[CH_R], rr)

    unpack(rr)
    stacked = dot(combine_parts, xe[...])
    mix = stacked[:rows] + stacked[rows : 2 * rows] + stacked[2 * rows :]
    for j in range(tp):
        fs[j] = mix[:, j * cols : (j + 1) * cols].astype(BF16)
    fr[pl.ds(me_t, 1)] = fs[pl.ds(me_t, 1)]
    send("tp", me_t, tp, CH_F, lambda j: fs.at[j], fr)
    wait_all(tp, rsem.at[CH_F], fr)
    out_ref[...] = (mixed.astype(F32) + jnp.sum(fr[...].astype(F32), axis=0)).astype(BF16)

    for channel, n, buf in (
        (CH_X, ep, xs), (CH_Q, ep, qs), (CH_KV, ep, kvs), (CH_O, tp, os_),
        (CH_M, tp, mr), (CH_D, ep, ds_), (CH_R, ep, rs), (CH_F, tp, fs),
    ):
        wait_all(n, ssem.at[channel], buf)


def local(ep, tp, tokens, norm_gain, w_query, w_key, w_value, w_forget, forget_bias, query_gain,
          key_gain, cache_keys, cache_values, cache_gates, lengths, w_output, ffn_gain, routes,
          route_weights, w_gate, w_up, w_down):
    rows, width = tokens.shape
    span, hd = cache_keys.shape[2], cache_keys.shape[3]
    depth = w_query.shape[0]
    cols = width // tp
    hidden = w_gate.shape[2]
    heads = w_forget.shape[1]
    n_blocks = width // LANES
    packed = (ep, 2 * CAP * n_blocks, LANES)
    vmem = pltpu.VMEM
    scratch = [
        vmem((rows, width), BF16), vmem((1, width), F32), vmem((depth, 3 * hd), BF16),
        vmem((heads, width), BF16), vmem((1, heads), F32), vmem((1, hd), F32), vmem((1, hd), F32),
        vmem((rows, span, hd), BF16), vmem((rows, span, hd), BF16), vmem((rows, 1, span), F32),
        vmem((1, rows), jnp.int32), vmem((hd, width), BF16), vmem((1, width), F32),
        vmem((2, rows), jnp.int32), vmem((2, rows), F32), vmem((width, 4 * hidden), BF16),
        vmem((2 * hidden, width), BF16),
        vmem((ep, rows, depth), BF16), vmem((ep, rows, depth), BF16),
        vmem((ep, rows, hd), F32), vmem((ep, rows, hd), F32),
        vmem((ep, 2 * rows, hd), BF16), vmem((ep, 2 * rows, hd), BF16),
        vmem((tp, rows, cols), F32), vmem((tp, rows, cols), F32),
        vmem((rows, cols), BF16), vmem((tp, rows, cols), BF16),
        vmem(packed, BF16), vmem(packed, BF16), vmem(packed, BF16), vmem(packed, BF16),
        vmem((tp, rows, cols), BF16), vmem((tp, rows, cols), BF16),
        vmem((n_blocks, 2 * CAP * ep, LANES), F32), vmem((2 * CAP * ep, width), BF16),
        pltpu.SemaphoreType.DMA((32,)), pltpu.SemaphoreType.DMA((8,)),
        pltpu.SemaphoreType.DMA((8,)),
    ]
    operands = (
        tokens, norm_gain[None], w_query, w_key, w_value, w_forget.T, forget_bias[None],
        query_gain[None], key_gain[None], cache_keys, cache_values, cache_gates, lengths[None],
        w_output, ffn_gain[None], routes.T, route_weights.T, w_gate, w_up, w_down,
    )
    return pl.pallas_call(
        functools.partial(kernel, ep, tp),
        out_shape=jax.ShapeDtypeStruct((rows, cols), BF16),
        in_specs=[pl.BlockSpec(memory_space=pl.ANY)] * len(operands),
        out_specs=pl.BlockSpec(memory_space=pltpu.VMEM),
        scratch_shapes=scratch,
        compiler_params=pltpu.CompilerParams(
            collective_id=0, has_side_effects=True, vmem_limit_bytes=48 * 1024 * 1024
        ),
        name="layer",
    )(*operands)


def solution(mesh):
    placed = (
        P("ep", None), P(), P("ep", "tp"), P("ep", "tp"), P("ep", "tp"), P(), P(), P(), P(),
        P("ep", "tp", None, None), P("ep", "tp", None, None), P("ep", "tp", None), P("ep"),
        P("tp", None), P(), P("ep", None), P("ep", None), P("ep", None, "tp"),
        P("ep", None, "tp"), P("ep", "tp", None),
    )
    return jax.shard_map(
        functools.partial(local, mesh.shape["ep"], mesh.shape["tp"]),
        mesh=mesh, in_specs=placed, out_specs=P("ep", "tp"), check_vma=False,
    )
```

```python
import functools

import jax
import jax.numpy as jnp
from jax import lax
from jax.experimental import pallas as pl
from jax.experimental.pallas import tpu as pltpu
from jax.sharding import PartitionSpec as P

MESH = pl.DeviceIdType.MESH
F32 = jnp.float32
BF16 = jnp.bfloat16
EPS = 1e-06
CAP = 2
LANES = 128

CH_X, CH_Q, CH_KV, CH_O, CH_M, CH_D, CH_R, CH_F = range(8)


def norm(v, gain):
    return v * lax.rsqrt(jnp.mean(v * v, axis=-1, keepdims=True) + EPS) * gain


def dot(a, b):
    return jnp.dot(a, b, preferred_element_type=F32)


def dot_t(a, b):
    return lax.dot_general(a, b, (((1,), (1,)), ((), ())), preferred_element_type=F32)


def swap_halves(a, b):
    low = lax.broadcasted_iota(jnp.int32, a.shape, 1) < 4
    a_turned, b_turned = pltpu.roll(a, 4, 1), pltpu.roll(b, 4, 1)
    return jnp.where(low, a, b_turned), jnp.where(low, a_turned, b)


def far_first(me, outer, inner):
    def hops(step):
        return min(step[0], outer - step[0]) + min(step[1], inner - step[1])

    steps = [(a, b) for a in range(outer) for b in range(inner) if a or b]
    a_me, b_me = lax.div(me, inner), lax.rem(me, inner)
    return [
        lax.rem(a_me + a, outer) * inner + lax.rem(b_me + b, inner)
        for a, b in sorted(steps, key=lambda step: -hops(step))
    ]


def kernel(ep, tp, *refs):
    names = (
        "tokens", "norm_gain", "wq", "wk", "wv", "wf", "f_bias", "q_gain", "k_gain", "keys",
        "values", "gates", "lengths", "wo", "ffn_gain", "routes", "r_weights", "wg", "wu", "wd",
    )
    hbm = dict(zip(names, refs))
    out_ref = refs[len(names)]
    (
        tok_v, ng_v, wqkv_v, wf_v, fb_v, qg_v, kg_v, k_v, v_v, g_v, len_v,
        wo_v, fg_v, rt_v, rw_v, wgu_v, wd_v,
        xs, xr, qs, qr, kvs, kvr, os_, or_, ms, mr, ds_, dr, rs, rr, fs, fr,
        big, xe,
        hsem, ssem, rsem,
    ) = refs[len(names) + 1 :]

    me_e, me_t = lax.axis_index("ep"), lax.axis_index("tp")
    rows, width = tok_v.shape
    span, hd = k_v.shape[1], k_v.shape[2]
    n_blocks = width // LANES
    depth = xs.shape[2]
    slots = 2 * CAP
    n_slots = ep * slots

    peers = {"ep": far_first(me_e, ep // 4, 4), "tp": far_first(me_t, tp // 2, 2)}
    barrier = pltpu.get_barrier_semaphore()
    for axis in ("ep", "tp"):
        for peer in peers[axis]:
            pl.semaphore_signal(barrier, inc=1, device_id={axis: peer}, device_id_type=MESH)

    fetches = {}

    def fetch(name, pairs):
        fetches[name] = []
        for src, dst in pairs:
            at = sum(len(f) for f in fetches.values())
            copy = pltpu.make_async_copy(src, dst, hsem.at[at])
            copy.start()
            fetches[name].append(copy)

    def need(*which):
        for name in which:
            for copy in fetches[name]:
                copy.wait()

    fetch("tok", [(hbm["tokens"], tok_v), (hbm["norm_gain"], ng_v)])
    fetch(
        "wqkv",
        [(hbm[w], wqkv_v.at[:, pl.ds(i * hd, hd)]) for i, w in enumerate(("wq", "wk", "wv"))],
    )
    fetch(
        "small",
        [
            (hbm["wf"], wf_v), (hbm["f_bias"], fb_v), (hbm["q_gain"], qg_v),
            (hbm["k_gain"], kg_v), (hbm["gates"], g_v), (hbm["lengths"], len_v),
            (hbm["ffn_gain"], fg_v), (hbm["routes"], rt_v), (hbm["r_weights"], rw_v),
        ],
    )
    quarter = rows // 4
    fetch(
        "k",
        [(hbm["keys"].at[pl.ds(i * quarter, quarter), 0], k_v.at[pl.ds(i * quarter, quarter)]) for i in range(4)],
    )
    fetch(
        "v",
        [(hbm["values"].at[pl.ds(i * quarter, quarter), 0], v_v.at[pl.ds(i * quarter, quarter)]) for i in range(4)],
    )
    fetch("wo", [(hbm["wo"], wo_v)])
    hidden = hbm["wg"].shape[2]
    fetch(
        "wgu",
        [
            (hbm[w].at[x], wgu_v.at[:, pl.ds((2 * x + i) * hidden, hidden)])
            for x in range(2)
            for i, w in enumerate(("wg", "wu"))
        ],
    )
    fetch("wd", [(hbm["wd"].at[x], wd_v.at[pl.ds(x * hidden, hidden)]) for x in range(2)])

    def send(axis, channel, src, dst):
        me = lax.axis_index(axis)
        for peer in peers[axis]:
            pltpu.make_async_remote_copy(
                src_ref=src(peer),
                dst_ref=dst.at[me],
                send_sem=ssem.at[channel],
                recv_sem=rsem.at[channel],
                device_id={axis: peer},
                device_id_type=MESH,
            ).start()

    def wait_all(n, sem, buf):
        part = buf.at[pl.ds(0, n - 1)]
        pltpu.make_async_copy(part, part, sem).wait()

    need("tok")
    normed = norm(tok_v[...].astype(F32), ng_v[...]).astype(BF16)
    for j in range(ep):
        xs[j] = normed[:, j * depth : (j + 1) * depth]
    xr[pl.ds(me_e, 1)] = xs[pl.ds(me_e, 1)]
    pl.semaphore_wait(barrier, ep + tp - 2)
    send("ep", CH_X, lambda j: xs.at[j], xr)

    need("small")
    row = lax.broadcasted_iota(jnp.int32, (rows, 1), 0)
    diagonal = lax.broadcasted_iota(jnp.int32, (rows, rows), 0) == lax.broadcasted_iota(
        jnp.int32, (rows, rows), 1
    )

    def as_column(line):
        return jnp.sum(jnp.where(diagonal, line, jnp.zeros_like(line)), axis=1, keepdims=True)

    biased = dot_t(normed, wf_v[...]) + fb_v[...]
    own_head = lax.broadcasted_iota(jnp.int32, biased.shape, 1) == me_t
    biased = jnp.sum(jnp.where(own_head, biased, 0.0), axis=1, keepdims=True)
    forget = jnp.minimum(biased, 0.0) - jnp.log1p(jnp.exp(-jnp.abs(biased)))

    lengths = as_column(len_v[...].astype(F32)).astype(jnp.int32)
    position = lax.broadcasted_iota(jnp.int32, (rows, span), 1)
    gates = jnp.zeros((rows, span), F32)
    for s in range(rows):
        gates = jnp.where(row == s, g_v[s], gates)
    last_gate = jnp.sum(jnp.where(position == lengths - 1, gates, 0.0), axis=1, keepdims=True)
    live = position < lengths

    first = rt_v[0:1, :]
    second = rt_v[1:2, :]
    slot_col = lax.broadcasted_iota(jnp.int32, (n_slots, rows), 0)
    expert_col, copy_col = lax.div(slot_col, CAP), lax.rem(slot_col, CAP)
    named = ((expert_col == first) | (expert_col == second)).astype(F32)
    before = (
        lax.broadcasted_iota(jnp.int32, (rows, rows), 0)
        < lax.broadcasted_iota(jnp.int32, (rows, rows), 1)
    ).astype(F32)
    earlier = dot(named.astype(BF16), before.astype(BF16))
    placing = jnp.where(earlier == copy_col.astype(F32), named, 0.0).astype(BF16)

    weight_sum = rw_v[0:1, :] + rw_v[1:2, :]
    share_a = as_column(rw_v[0:1, :] / weight_sum)
    share_b = as_column(rw_v[1:2, :] / weight_sum)
    route_a = as_column(first.astype(F32)).astype(jnp.int32)
    route_b = as_column(second.astype(F32)).astype(jnp.int32)
    slot_row = lax.broadcasted_iota(jnp.int32, (rows, n_slots), 1)
    expert_row, copy_row = lax.div(slot_row, CAP), lax.rem(slot_row, CAP)
    is_a, is_b = expert_row == route_a, expert_row == route_b
    after = (
        lax.broadcasted_iota(jnp.int32, (rows, rows), 1)
        < lax.broadcasted_iota(jnp.int32, (rows, rows), 0)
    ).astype(BF16)
    earlier_row = dot(after, (is_a | is_b).astype(F32).astype(BF16))
    combine = jnp.where(is_a, share_a, 0.0) + jnp.where(is_b, share_b, 0.0)
    combine = jnp.where(earlier_row == copy_row.astype(F32), combine, 0.0)
    combine_1 = combine.astype(BF16)
    rest = combine - combine_1.astype(F32)
    combine_2 = rest.astype(BF16)
    combine_3 = (rest - combine_2.astype(F32)).astype(BF16)
    combine_parts = jnp.concatenate([combine_1, combine_2, combine_3], axis=0)

    need("wqkv")
    wait_all(ep, rsem.at[CH_X], xr)
    part = dot(xr[...].reshape(ep * rows, depth), wqkv_v[...])
    qs[...] = part[:, :hd].reshape(ep, rows, hd)
    for j in range(ep):
        own = part[j * rows : (j + 1) * rows]
        kvs[j, 0:rows, :] = own[:, hd : 2 * hd].astype(BF16)
        kvs[j, rows : 2 * rows, :] = own[:, 2 * hd :].astype(BF16)
    qr[pl.ds(me_e, 1)] = qs[pl.ds(me_e, 1)]
    kvr[pl.ds(me_e, 1)] = kvs[pl.ds(me_e, 1)]
    send("ep", CH_Q, lambda j: qs.at[j], qr)
    send("ep", CH_KV, lambda j: kvs.at[j], kvr)
    need("k", "v")
    wait_all(ep, rsem.at[CH_Q], qr)
    queries = norm(jnp.sum(qr[...], axis=0), qg_v[...]).astype(BF16)

    score_scale = hd ** (-0.5)
    scores = jnp.zeros((rows, span), F32)
    for s in range(rows):
        scores = jnp.where(row == s, dot_t(queries, k_v[s]), scores)
    wait_all(ep, rsem.at[CH_KV], kvr)
    kv_raw = jnp.sum(kvr[...].astype(F32), axis=0)
    keys_new = norm(kv_raw[:rows], kg_v[...]).astype(BF16)
    values_new = kv_raw[rows:].astype(BF16)
    scores = scores * score_scale + (last_gate - gates) + forget
    scores = jnp.where(live, scores, -1e30)
    own_score = (
        jnp.sum(queries.astype(F32) * keys_new.astype(F32), axis=1, keepdims=True) * score_scale
    )
    peak = jnp.maximum(jnp.max(scores, axis=1, keepdims=True), own_score)
    weights = jnp.exp(scores - peak)
    own_weight = jnp.exp(own_score - peak)
    denominator = jnp.sum(weights, axis=1, keepdims=True) + own_weight
    probabilities = weights / denominator
    own_prob = (own_weight / denominator).astype(BF16).astype(F32)
    attended = own_prob * values_new.astype(F32)
    for s in range(rows):
        mine = jnp.where(row == s, probabilities, 0.0).astype(BF16)
        attended = attended + dot(mine, v_v[s])
    attended = attended.astype(BF16)

    need("wo")
    cols = or_.shape[2]
    partial = dot(attended, wo_v[...])
    for j in range(tp):
        os_[j] = partial[:, j * cols : (j + 1) * cols].astype(BF16)
    or_[pl.ds(me_t, 1)] = os_[pl.ds(me_t, 1)]
    send("tp", CH_O, lambda j: os_.at[j], or_)
    wait_all(tp, rsem.at[CH_O], or_)
    own_tokens = tok_v[:, pl.ds(pl.multiple_of(me_t * cols, cols), cols)].astype(F32)
    mixed = (own_tokens + jnp.sum(or_[...].astype(F32), axis=0)).astype(BF16)
    ms[...] = mixed
    mr[pl.ds(me_t, 1)] = mixed[None]
    send("tp", CH_M, lambda j: ms, mr)
    need("wgu", "wd")
    wait_all(tp, rsem.at[CH_M], mr)

    squares = jnp.zeros((rows, 1), F32)
    for b in range(n_blocks):
        block = mr[b].astype(F32)
        squares = squares + jnp.sum(block * block, axis=1, keepdims=True)
    factor = lax.rsqrt(squares / width + EPS)
    for b in range(n_blocks):
        block = mr[b].astype(F32) * factor * fg_v[:, b * LANES : (b + 1) * LANES]
        big[b] = dot(placing, block.astype(BF16))

    def pack(dst):
        for pair in range(ep // 2):
            tile = big[:, pair * 8 : pair * 8 + 8, :].reshape(n_blocks // 2, 2, 8, LANES)
            even, odd = swap_halves(tile[:, 0], tile[:, 1])
            dst[2 * pair] = even.reshape(n_blocks * 4, LANES).astype(BF16)
            dst[2 * pair + 1] = odd.reshape(n_blocks * 4, LANES).astype(BF16)

    def unpack(src):
        for quad in range(ep // 4):
            halves = []
            for pair in (2 * quad, 2 * quad + 1):
                a = src[2 * pair].astype(F32).reshape(n_blocks // 2, 8, LANES)
                b = src[2 * pair + 1].astype(F32).reshape(n_blocks // 2, 8, LANES)
                halves.append(swap_halves(a, b))
            for odd in range(2):
                whole = jnp.concatenate([halves[0][odd], halves[1][odd]], axis=1).astype(BF16)
                for i in range(n_blocks // 2):
                    b = 2 * i + odd
                    xe[quad * 16 : quad * 16 + 16, b * LANES : (b + 1) * LANES] = whole[i]

    pack(ds_)
    dr[pl.ds(me_e, 1)] = ds_[pl.ds(me_e, 1)]
    send("ep", CH_D, lambda j: ds_.at[j], dr)
    wait_all(ep, rsem.at[CH_D], dr)

    unpack(dr)
    both = dot(xe[...], wgu_v[...])
    kind = lax.div(lax.rem(lax.broadcasted_iota(jnp.int32, (n_slots, 1), 0), slots), CAP)
    parts = []
    for x in range(2):
        gate = both[:, 2 * x * hidden : (2 * x + 1) * hidden]
        upper = both[:, (2 * x + 1) * hidden : (2 * x + 2) * hidden]
        parts.append(jnp.where(kind == x, gate * jax.nn.sigmoid(gate) * upper, 0.0))
    hidden_rows = jnp.concatenate(parts, axis=1).astype(BF16)
    expert_rows = dot(hidden_rows, wd_v[...])
    for b in range(n_blocks):
        big[b] = expert_rows[:, b * LANES : (b + 1) * LANES]
    pack(rs)
    rr[pl.ds(me_e, 1)] = rs[pl.ds(me_e, 1)]
    send("ep", CH_R, lambda j: rs.at[j], rr)
    wait_all(ep, rsem.at[CH_R], rr)

    unpack(rr)
    stacked = dot(combine_parts, xe[...])
    mix = stacked[:rows] + stacked[rows : 2 * rows] + stacked[2 * rows :]
    for j in range(tp):
        fs[j] = mix[:, j * cols : (j + 1) * cols].astype(BF16)
    fr[pl.ds(me_t, 1)] = fs[pl.ds(me_t, 1)]
    send("tp", CH_F, lambda j: fs.at[j], fr)
    wait_all(tp, rsem.at[CH_F], fr)
    out_ref[...] = (mixed.astype(F32) + jnp.sum(fr[...].astype(F32), axis=0)).astype(BF16)

    for channel, n, buf in (
        (CH_X, ep, xs), (CH_Q, ep, qs), (CH_KV, ep, kvs), (CH_O, tp, os_),
        (CH_M, tp, mr), (CH_D, ep, ds_), (CH_R, ep, rs), (CH_F, tp, fs),
    ):
        wait_all(n, ssem.at[channel], buf)


def local(ep, tp, tokens, norm_gain, w_query, w_key, w_value, w_forget, forget_bias, query_gain,
          key_gain, cache_keys, cache_values, cache_gates, lengths, w_output, ffn_gain, routes,
          route_weights, w_gate, w_up, w_down):
    rows, width = tokens.shape
    span, hd = cache_keys.shape[2], cache_keys.shape[3]
    depth = w_query.shape[0]
    cols = width // tp
    hidden = w_gate.shape[2]
    heads = w_forget.shape[1]
    n_blocks = width // LANES
    packed = (ep, 2 * CAP * n_blocks, LANES)
    vmem = pltpu.VMEM
    scratch = [
        vmem((rows, width), BF16), vmem((1, width), F32), vmem((depth, 3 * hd), BF16),
        vmem((heads, width), BF16), vmem((1, heads), F32), vmem((1, hd), F32), vmem((1, hd), F32),
        vmem((rows, span, hd), BF16), vmem((rows, span, hd), BF16), vmem((rows, 1, span), F32),
        vmem((1, rows), jnp.int32), vmem((hd, width), BF16), vmem((1, width), F32),
        vmem((2, rows), jnp.int32), vmem((2, rows), F32), vmem((width, 4 * hidden), BF16),
        vmem((2 * hidden, width), BF16),
        vmem((ep, rows, depth), BF16), vmem((ep, rows, depth), BF16),
        vmem((ep, rows, hd), F32), vmem((ep, rows, hd), F32),
        vmem((ep, 2 * rows, hd), BF16), vmem((ep, 2 * rows, hd), BF16),
        vmem((tp, rows, cols), BF16), vmem((tp, rows, cols), BF16),
        vmem((rows, cols), BF16), vmem((tp, rows, cols), BF16),
        vmem(packed, BF16), vmem(packed, BF16), vmem(packed, BF16), vmem(packed, BF16),
        vmem((tp, rows, cols), BF16), vmem((tp, rows, cols), BF16),
        vmem((n_blocks, 2 * CAP * ep, LANES), F32), vmem((2 * CAP * ep, width), BF16),
        pltpu.SemaphoreType.DMA((32,)), pltpu.SemaphoreType.DMA((8,)),
        pltpu.SemaphoreType.DMA((8,)),
    ]
    operands = (
        tokens, norm_gain[None], w_query, w_key, w_value, w_forget.T, forget_bias[None],
        query_gain[None], key_gain[None], cache_keys, cache_values, cache_gates, lengths[None],
        w_output, ffn_gain[None], routes.T, route_weights.T, w_gate, w_up, w_down,
    )
    return pl.pallas_call(
        functools.partial(kernel, ep, tp),
        out_shape=jax.ShapeDtypeStruct((rows, cols), BF16),
        in_specs=[pl.BlockSpec(memory_space=pltpu.HBM)] * len(operands),
        out_specs=pl.BlockSpec(memory_space=pltpu.VMEM),
        scratch_shapes=scratch,
        compiler_params=pltpu.CompilerParams(
            collective_id=0, has_side_effects=True, vmem_limit_bytes=67043328
        ),
        name="layer",
    )(*operands)


def solution(mesh):
    placed = (
        P("ep", None), P(), P("ep", "tp"), P("ep", "tp"), P("ep", "tp"), P(), P(), P(), P(),
        P("ep", "tp", None, None), P("ep", "tp", None, None), P("ep", "tp", None), P("ep"),
        P("tp", None), P(), P("ep", None), P("ep", None), P("ep", None, "tp"),
        P("ep", None, "tp"), P("ep", "tp", None),
    )
    return jax.shard_map(
        functools.partial(local, mesh.shape["ep"], mesh.shape["tp"]),
        mesh=mesh, in_specs=placed, out_specs=P("ep", "tp"), check_vma=False,
    )
```

```python
import functools
import itertools

import jax
import jax.numpy as jnp
from jax import lax
from jax.experimental import pallas as pl
from jax.experimental.pallas import tpu as pltpu
from jax.sharding import PartitionSpec as P

MESH = pl.DeviceIdType.MESH
F32 = jnp.float32
BF16 = jnp.bfloat16
EPS = 1e-06
CAP = 2
LANES = 128

CH_X, CH_Q, CH_KV, CH_O, CH_D, CH_DP, CH_RP, CH_R = range(8)


def norm(v, gain):
    return v * lax.rsqrt(jnp.mean(v * v, axis=-1, keepdims=True) + EPS) * gain


def dot(a, b):
    return jnp.dot(a, b, preferred_element_type=F32)


def dot_t(a, b):
    return lax.dot_general(a, b, (((1,), (1,)), ((), ())), preferred_element_type=F32)


def far_first(*sizes):
    steps = itertools.product(*(range(size) for size in sizes))
    steps = sorted(steps, key=lambda step: -sum(min(a, n - a) for a, n in zip(step, sizes)))
    return steps[:-1]


def moved(me, size, step):
    return lax.rem(me + step, size) if step else me


def kernel(ep, tp, *refs):
    names = (
        "tokens", "norm_gain", "wq", "wk", "wv", "wf", "f_bias", "q_gain", "k_gain", "keys",
        "values", "gates", "lengths", "wo", "ffn_gain", "routes", "r_weights", "wg", "wu", "wd",
    )
    hbm = dict(zip(names, refs))
    out_ref = refs[len(names)]
    (
        tok_v, ng_v, wqkv_v, wf_v, fb_v, qg_v, kg_v, k_v, v_v, g_v, len_v,
        wo_v, fg_v, rt_v, rw_v, wgu_v, wd_v,
        xs, xr, qs, qr, kvs, kvr, os_, or_, ds_, dr, dw, dp, rg, rp, rs, rr, big, xe,
        hsem, ssem, rsem,
    ) = refs[len(names) + 1 :]

    me_e, me_t = lax.axis_index("ep"), lax.axis_index("tp")
    rows, width = tok_v.shape
    span, hd = k_v.shape[1], k_v.shape[2] // 2
    depth = xs.shape[2]
    slots = 2 * CAP
    n_slots = ep * slots

    outer, chips = ep // 4, tp // 2
    y, x = lax.div(me_e, 4), lax.rem(me_e, 4)
    z, core = lax.div(me_t, 2), lax.rem(me_t, 2)
    y_at = [moved(y, outer, a) for a in range(outer)]
    x_at = [moved(x, 4, a) for a in range(4)]
    z_at = [moved(z, chips, a) for a in range(chips)]
    core_at = [core, 1 - core]
    peers = {
        "ep": [y_at[a] * 4 + x_at[b] for a, b in far_first(outer, 4)],
        "tp": [z_at[a] * 2 + core_at[b] for a, b in far_first(chips, 2)],
    }
    barrier = pltpu.get_barrier_semaphore()
    for axis in ("ep", "tp"):
        for peer in peers[axis]:
            pl.semaphore_signal(barrier, inc=1, device_id={axis: peer}, device_id_type=MESH)

    fetches = {}

    def fetch(name, pairs):
        fetches[name] = []
        for src, dst in pairs:
            at = sum(len(f) for f in fetches.values())
            copy = pltpu.make_async_copy(src, dst, hsem.at[at])
            copy.start()
            fetches[name].append(copy)

    def need(*which):
        for name in which:
            for copy in fetches[name]:
                copy.wait()

    fetch("tok", [(hbm["tokens"], tok_v), (hbm["norm_gain"], ng_v)])
    fetch(
        "wqkv",
        [(hbm[w], wqkv_v.at[:, pl.ds(i * hd, hd)]) for i, w in enumerate(("wq", "wk", "wv"))],
    )
    fetch(
        "small",
        [
            (hbm["wf"], wf_v), (hbm["f_bias"], fb_v), (hbm["q_gain"], qg_v),
            (hbm["k_gain"], kg_v), (hbm["gates"], g_v), (hbm["lengths"], len_v),
            (hbm["ffn_gain"], fg_v), (hbm["routes"], rt_v), (hbm["r_weights"], rw_v),
        ],
    )
    for name, src, dst in (("k", "keys", k_v), ("v", "values", v_v)):
        fetch(
            name,
            [
                (hbm[src].at[s, 0], dst.at[s // 2, :, pl.ds((s % 2) * hd, hd)])
                for s in range(rows)
            ],
        )
    fetch("wo", [(hbm["wo"], wo_v)])
    hidden = hbm["wg"].shape[2]
    fetch(
        "wgu",
        [
            (hbm[w].at[x], wgu_v.at[:, pl.ds((2 * x + i) * hidden, hidden)])
            for x in range(2)
            for i, w in enumerate(("wg", "wu"))
        ],
    )
    fetch("wd", [(hbm["wd"].at[x], wd_v.at[pl.ds(x * hidden, hidden)]) for x in range(2)])

    def send(axis, channel, src, dst):
        me = lax.axis_index(axis)
        for peer in peers[axis]:
            pltpu.make_async_remote_copy(
                src_ref=src(peer),
                dst_ref=dst.at[me],
                send_sem=ssem.at[channel],
                recv_sem=rsem.at[channel],
                device_id={axis: peer},
                device_id_type=MESH,
            ).start()

    def wait_all(n, sem, buf):
        part = buf.at[pl.ds(0, n - 1)]
        pltpu.make_async_copy(part, part, sem).wait()

    need("tok")
    normed = norm(tok_v[...].astype(F32), ng_v[...]).astype(BF16)
    for j in range(ep):
        xs[j] = normed[:, j * depth : (j + 1) * depth]
    xr[pl.ds(me_e, 1)] = xs[pl.ds(me_e, 1)]
    pl.semaphore_wait(barrier, ep + tp - 2)
    send("ep", CH_X, lambda j: xs.at[j], xr)

    need("small")
    row = lax.broadcasted_iota(jnp.int32, (rows, 1), 0)
    diagonal = lax.broadcasted_iota(jnp.int32, (rows, rows), 0) == lax.broadcasted_iota(
        jnp.int32, (rows, rows), 1
    )

    def as_column(line):
        return jnp.sum(jnp.where(diagonal, line, jnp.zeros_like(line)), axis=1, keepdims=True)

    biased = dot_t(normed, wf_v[...]) + fb_v[...]
    own_head = lax.broadcasted_iota(jnp.int32, biased.shape, 1) == me_t
    biased = jnp.sum(jnp.where(own_head, biased, 0.0), axis=1, keepdims=True)
    forget = jnp.minimum(biased, 0.0) - jnp.log1p(jnp.exp(-jnp.abs(biased)))

    lengths = as_column(len_v[...].astype(F32)).astype(jnp.int32)
    position = lax.broadcasted_iota(jnp.int32, (rows, span), 1)
    gates = jnp.zeros((rows, span), F32)
    for s in range(rows):
        gates = jnp.where(row == s, g_v[s], gates)
    last_gate = jnp.sum(jnp.where(position == lengths - 1, gates, 0.0), axis=1, keepdims=True)
    live = position < lengths

    first = rt_v[0:1, :]
    second = rt_v[1:2, :]
    slot_col = lax.broadcasted_iota(jnp.int32, (n_slots, rows), 0)
    expert_col, copy_col = lax.div(slot_col, CAP), lax.rem(slot_col, CAP)
    named = ((expert_col == first) | (expert_col == second)).astype(F32)
    before = (
        lax.broadcasted_iota(jnp.int32, (rows, rows), 0)
        < lax.broadcasted_iota(jnp.int32, (rows, rows), 1)
    ).astype(F32)
    earlier = dot(named.astype(BF16), before.astype(BF16))
    placing = jnp.where(earlier == copy_col.astype(F32), named, 0.0).astype(BF16)

    weight_sum = rw_v[0:1, :] + rw_v[1:2, :]
    share_a = as_column(rw_v[0:1, :] / weight_sum)
    share_b = as_column(rw_v[1:2, :] / weight_sum)
    route_a = as_column(first.astype(F32)).astype(jnp.int32)
    route_b = as_column(second.astype(F32)).astype(jnp.int32)
    slot_row = lax.broadcasted_iota(jnp.int32, (rows, n_slots), 1)
    expert_row, copy_row = lax.div(slot_row, CAP), lax.rem(slot_row, CAP)
    is_a, is_b = expert_row == route_a, expert_row == route_b
    after = (
        lax.broadcasted_iota(jnp.int32, (rows, rows), 1)
        < lax.broadcasted_iota(jnp.int32, (rows, rows), 0)
    ).astype(BF16)
    earlier_row = dot(after, (is_a | is_b).astype(F32).astype(BF16))
    combine = jnp.where(is_a, share_a, 0.0) + jnp.where(is_b, share_b, 0.0)
    combine = jnp.where(earlier_row == copy_row.astype(F32), combine, 0.0)
    combine_1 = combine.astype(BF16)
    rest = combine - combine_1.astype(F32)
    combine_2 = rest.astype(BF16)
    combine_3 = (rest - combine_2.astype(F32)).astype(BF16)
    combine_parts = jnp.concatenate([combine_1, combine_2, combine_3], axis=0)

    need("wqkv")
    wait_all(ep, rsem.at[CH_X], xr)
    part = dot(xr[...].reshape(ep * rows, depth), wqkv_v[...])
    qs[...] = part[:, :hd].reshape(ep, rows, hd)
    for j in range(ep):
        own = part[j * rows : (j + 1) * rows]
        kvs[j, 0:rows, :] = own[:, hd : 2 * hd].astype(BF16)
        kvs[j, rows : 2 * rows, :] = own[:, 2 * hd :].astype(BF16)
    qr[pl.ds(me_e, 1)] = qs[pl.ds(me_e, 1)]
    kvr[pl.ds(me_e, 1)] = kvs[pl.ds(me_e, 1)]
    send("ep", CH_Q, lambda j: qs.at[j], qr)
    send("ep", CH_KV, lambda j: kvs.at[j], kvr)
    need("k", "v")
    wait_all(ep, rsem.at[CH_Q], qr)
    queries = norm(jnp.sum(qr[...], axis=0), qg_v[...]).astype(BF16)

    score_scale = hd ** (-0.5)
    wide = queries.astype(F32)
    scores = jnp.zeros((rows, span), F32)
    for pair in range(rows // 2):
        both = [jnp.where(row == 2 * pair + i, wide, 0.0) for i in range(2)]
        scores = scores + dot_t(jnp.concatenate(both, axis=1).astype(BF16), k_v[pair])
    wait_all(ep, rsem.at[CH_KV], kvr)
    kv_raw = jnp.sum(kvr[...].astype(F32), axis=0)
    keys_new = norm(kv_raw[:rows], kg_v[...]).astype(BF16)
    values_new = kv_raw[rows:].astype(BF16)
    scores = scores * score_scale + (last_gate - gates) + forget
    scores = jnp.where(live, scores, -1e30)
    own_score = (
        jnp.sum(queries.astype(F32) * keys_new.astype(F32), axis=1, keepdims=True) * score_scale
    )
    peak = jnp.maximum(jnp.max(scores, axis=1, keepdims=True), own_score)
    weights = jnp.exp(scores - peak)
    own_weight = jnp.exp(own_score - peak)
    denominator = jnp.sum(weights, axis=1, keepdims=True) + own_weight
    probabilities = weights / denominator
    own_prob = (own_weight / denominator).astype(BF16).astype(F32)
    summed = jnp.zeros((rows, 2 * hd), F32)
    for pair in range(rows // 2):
        mine = jnp.where(lax.div(row, 2) == pair, probabilities, 0.0).astype(BF16)
        summed = summed + dot(mine, v_v[pair])
    summed = jnp.where(lax.rem(row, 2) == 0, summed[:, :hd], summed[:, hd:])
    attended = (summed + own_prob * values_new.astype(F32)).astype(BF16)

    need("wo")
    cols = or_.shape[2]
    partial = dot(attended, wo_v[...])
    for j in range(tp):
        os_[j] = partial[:, j * cols : (j + 1) * cols].astype(BF16)
    or_[pl.ds(me_t, 1)] = os_[pl.ds(me_t, 1)]
    send("tp", CH_O, lambda j: os_.at[j], or_)
    wait_all(tp, rsem.at[CH_O], or_)
    own_tokens = tok_v[:, pl.ds(pl.multiple_of(me_t * cols, cols), cols)].astype(F32)
    mixed = (own_tokens + jnp.sum(or_[...].astype(F32), axis=0)).astype(BF16)

    def send_grid(channel, src, dst):
        for a, b, d in far_first(outer, 4, chips):
            owner = y_at[a] * 4 + x_at[b]
            pltpu.make_async_remote_copy(
                src_ref=src(owner, z_at[d]),
                dst_ref=dst.at[pl.ds(z * n_slots + slots * me_e, slots)],
                send_sem=ssem.at[channel],
                recv_sem=rsem.at[channel],
                device_id={"ep": owner, "tp": z_at[d] * 2 + core},
                device_id_type=MESH,
            ).start()

    def wait_grid(sem, buf):
        part = buf.at[pl.ds(0, (ep * chips - 1) * slots)]
        pltpu.make_async_copy(part, part, sem).wait()

    def to_partner(channel, src, dst):
        copy = pltpu.make_async_remote_copy(
            src_ref=src,
            dst_ref=dst,
            send_sem=ssem.at[channel],
            recv_sem=rsem.at[channel],
            device_id={"tp": z * 2 + 1 - core},
            device_id_type=MESH,
        )
        copy.start()
        return copy

    slot_line = lax.broadcasted_iota(jnp.int32, (n_slots, 1), 0)
    own_slots = lax.div(slot_line, slots) == me_e

    def part_of(buf, own, chip):
        got = buf[chip * n_slots : (chip + 1) * n_slots, :].astype(F32)
        return jnp.where(own_slots & (z == chip), own, got)

    placed = dot(placing, mixed)
    ds_[...] = placed.astype(BF16)
    send_grid(CH_D, lambda owner, chip: ds_.at[pl.ds(slots * owner, slots)], dr)
    need("wgu", "wd")
    wait_grid(rsem.at[CH_D], dr)
    squares = jnp.zeros((n_slots, LANES), F32)
    for chip in range(chips):
        block = part_of(dr, placed, chip)
        squares = squares + block * block
        dw[chip * n_slots : (chip + 1) * n_slots, :] = block.astype(BF16)
    swap = to_partner(CH_DP, dw, dp)
    swap.wait_recv()
    for chip in range(chips):
        block = dp[chip * n_slots : (chip + 1) * n_slots, :].astype(F32)
        squares = squares + block * block
    factor = lax.rsqrt(jnp.sum(squares, axis=1, keepdims=True) / width + EPS)
    for buf, owner in ((dw, core), (dp, 1 - core)):
        for chip in range(chips):
            at = pl.multiple_of((2 * chip + owner) * LANES, LANES)
            block = buf[chip * n_slots : (chip + 1) * n_slots, :].astype(F32)
            block = block * factor * fg_v[:, pl.ds(at, LANES)]
            xe[:, pl.ds(at, LANES)] = block.astype(BF16)

    both = dot(xe[...], wgu_v[...])
    kind = lax.div(lax.rem(slot_line, slots), CAP)
    parts = []
    for i in range(2):
        gate = both[:, 2 * i * hidden : (2 * i + 1) * hidden]
        upper = both[:, (2 * i + 1) * hidden : (2 * i + 2) * hidden]
        parts.append(jnp.where(kind == i, gate * jax.nn.sigmoid(gate) * upper, 0.0))
    hidden_rows = jnp.concatenate(parts, axis=1).astype(BF16)

    def down(chip, owner):
        at = pl.multiple_of((2 * chip + owner) * LANES, LANES)
        return dot(hidden_rows, wd_v[:, pl.ds(at, LANES)])

    for chip in range(chips):
        rg[chip * n_slots : (chip + 1) * n_slots, :] = down(chip, 1 - core).astype(BF16)
    give = to_partner(CH_RP, rg, rp)
    for chip in range(chips):
        big[chip * n_slots : (chip + 1) * n_slots, :] = down(chip, core)
    give.wait_recv()
    for chip in range(chips):
        at = slice(chip * n_slots, (chip + 1) * n_slots)
        rs[at, :] = (big[at, :] + rp[at, :].astype(F32)).astype(BF16)
    send_grid(CH_R, lambda owner, chip: rs.at[pl.ds(chip * n_slots + slots * owner, slots)], rr)
    wait_grid(rsem.at[CH_R], rr)

    own_rows = rs[pl.ds(pl.multiple_of(z * n_slots, n_slots), n_slots), :].astype(F32)
    total = jnp.zeros((n_slots, LANES), F32)
    for chip in range(chips):
        total = total + part_of(rr, own_rows, chip)
    stacked = dot(combine_parts, total.astype(BF16))
    mix = stacked[:rows] + stacked[rows : 2 * rows] + stacked[2 * rows :]
    out_ref[...] = (mixed.astype(F32) + mix).astype(BF16)

    for channel, n, buf in ((CH_X, ep, xs), (CH_Q, ep, qs), (CH_KV, ep, kvs), (CH_O, tp, os_)):
        wait_all(n, ssem.at[channel], buf)
    for channel, buf in ((CH_D, dr), (CH_R, rs)):
        wait_grid(ssem.at[channel], buf)
    swap.wait_send()
    give.wait_send()


def local(ep, tp, tokens, norm_gain, w_query, w_key, w_value, w_forget, forget_bias, query_gain,
          key_gain, cache_keys, cache_values, cache_gates, lengths, w_output, ffn_gain, routes,
          route_weights, w_gate, w_up, w_down):
    rows, width = tokens.shape
    span, hd = cache_keys.shape[2], cache_keys.shape[3]
    depth = w_query.shape[0]
    cols = width // tp
    hidden = w_gate.shape[2]
    heads = w_forget.shape[1]
    n_slots = 2 * CAP * ep
    vmem = pltpu.VMEM
    scratch = [
        vmem((rows, width), BF16), vmem((1, width), F32), vmem((depth, 3 * hd), BF16),
        vmem((heads, width), BF16), vmem((1, heads), F32), vmem((1, hd), F32), vmem((1, hd), F32),
        vmem((rows // 2, span, 2 * hd), BF16), vmem((rows // 2, span, 2 * hd), BF16), vmem((rows, 1, span), F32),
        vmem((1, rows), jnp.int32), vmem((hd, width), BF16), vmem((1, width), F32),
        vmem((2, rows), jnp.int32), vmem((2, rows), F32), vmem((width, 4 * hidden), BF16),
        vmem((2 * hidden, width), BF16),
        vmem((ep, rows, depth), BF16), vmem((ep, rows, depth), BF16),
        vmem((ep, rows, hd), F32), vmem((ep, rows, hd), F32),
        vmem((ep, 2 * rows, hd), BF16), vmem((ep, 2 * rows, hd), BF16),
        vmem((tp, rows, cols), BF16), vmem((tp, rows, cols), BF16),
        vmem((n_slots, LANES), BF16), *[vmem((tp // 2 * n_slots, LANES), BF16)] * 7,
        vmem((tp // 2 * n_slots, LANES), F32), vmem((n_slots, width), BF16),
        pltpu.SemaphoreType.DMA((64,)), pltpu.SemaphoreType.DMA((8,)),
        pltpu.SemaphoreType.DMA((8,)),
    ]
    operands = (
        tokens, norm_gain[None], w_query, w_key, w_value, w_forget.T, forget_bias[None],
        query_gain[None], key_gain[None], cache_keys, cache_values, cache_gates, lengths[None],
        w_output, ffn_gain[None], routes.T, route_weights.T, w_gate, w_up, w_down,
    )
    return pl.pallas_call(
        functools.partial(kernel, ep, tp),
        out_shape=jax.ShapeDtypeStruct((rows, cols), BF16),
        in_specs=[pl.BlockSpec(memory_space=pltpu.HBM)] * len(operands),
        out_specs=pl.BlockSpec(memory_space=pltpu.VMEM),
        scratch_shapes=scratch,
        compiler_params=pltpu.CompilerParams(
            collective_id=0, has_side_effects=True, vmem_limit_bytes=67043328
        ),
        name="layer",
    )(*operands)


def solution(mesh):
    placed = (
        P("ep", None), P(), P("ep", "tp"), P("ep", "tp"), P("ep", "tp"), P(), P(), P(), P(),
        P("ep", "tp", None, None), P("ep", "tp", None, None), P("ep", "tp", None), P("ep"),
        P("tp", None), P(), P("ep", None), P("ep", None), P("ep", None, "tp"),
        P("ep", None, "tp"), P("ep", "tp", None),
    )
    return jax.shard_map(
        functools.partial(local, mesh.shape["ep"], mesh.shape["tp"]),
        mesh=mesh, in_specs=placed, out_specs=P("ep", "tp"), check_vma=False,
    )
```

```python
import functools
import itertools

import jax
import jax.numpy as jnp
from jax import lax
from jax.experimental import pallas as pl
from jax.experimental.pallas import tpu as pltpu
from jax.sharding import PartitionSpec as P

MESH = pl.DeviceIdType.MESH
F32 = jnp.float32
BF16 = jnp.bfloat16
EPS = 1e-06
CAP = 2
LANES = 128

CH_X, CH_Q, CH_KV, CH_O, CH_R, CH_D, CH_DP, CH_RP = range(8)


def norm(v, gain):
    return v * lax.rsqrt(jnp.mean(v * v, axis=-1, keepdims=True) + EPS) * gain


def dot(a, b):
    return jnp.dot(a, b, preferred_element_type=F32)


def dot_t(a, b):
    return lax.dot_general(a, b, (((1,), (1,)), ((), ())), preferred_element_type=F32)


def hops(step, sizes):
    return sum(min(a, n - a) for a, n in zip(step, sizes))


def far_first(*sizes):
    steps = itertools.product(*(range(size) for size in sizes))
    return sorted(steps, key=lambda step: -hops(step, sizes))


def moved(me, size, step):
    return lax.rem(me + step, size) if step else me


def kernel(ep, tp, *refs):
    names = (
        "tokens", "norm_gain", "wq", "wk", "wv", "wf", "f_bias", "q_gain", "k_gain", "keys",
        "values", "gates", "lengths", "wo", "ffn_gain", "routes", "r_weights", "wg", "wu", "wd",
    )
    hbm = dict(zip(names, refs))
    out_ref = refs[len(names)]
    (
        tok_v, ng_v, wqkv_v, wf_v, fb_v, qg_v, kg_v, k_v, v_v, g_v, len_v,
        wo_v, fg_v, rt_v, rw_v, wgu_v, wd_v,
        xs, xr, qs, qr, kvs, kvr, os_, or_, ds_, dr, dp, rg, rp, rs, rr, kt, xe,
        hsem, ssem, rsem, dsem, dpsem, rpsem,
    ) = refs[len(names) + 1 :]

    me_e, me_t = lax.axis_index("ep"), lax.axis_index("tp")
    rows, width = tok_v.shape
    span, hd = k_v.shape[1], k_v.shape[2]
    depth = xs.shape[2]
    hidden = wd_v.shape[0] // 2
    slots = 2 * CAP
    n_slots = ep * slots

    outer, chips = ep // 4, tp // 2
    y, x = lax.div(me_e, 4), lax.rem(me_e, 4)
    z, core = lax.div(me_t, 2), lax.rem(me_t, 2)
    y_at = [moved(y, outer, a) for a in range(outer)]
    x_at = [moved(x, 4, a) for a in range(4)]
    z_at = [moved(z, chips, a) for a in range(chips)]
    core_at = [core, 1 - core]
    peers = {
        "ep": [y_at[a] * 4 + x_at[b] for a, b in far_first(outer, 4)[:-1]],
        "tp": [z_at[a] * 2 + core_at[b] for a, b in far_first(chips, 2)[:-1]],
    }
    partner = z * 2 + 1 - core
    chip_steps = [step for (step,) in far_first(chips)]
    chip_order = [z_at[step] for step in chip_steps]
    seen_as = {step: chip_steps.index(-step % chips) for step in chip_steps}
    barrier = pltpu.get_barrier_semaphore()
    for peer in peers["ep"]:
        pl.semaphore_signal(barrier, inc=1, device_id={"ep": peer}, device_id_type=MESH)
    for peer in peers["tp"]:
        pl.semaphore_signal(barrier, inc=1, device_id={"tp": peer}, device_id_type=MESH)

    fetches, taken = {}, itertools.count()

    def fetch(name, pairs, whole=None):
        waits, at = [], next(taken) if whole is not None else None
        for src, dst in pairs:
            sem = hsem.at[next(taken) if whole is None else at]
            copy = pltpu.make_async_copy(src, dst, sem)
            copy.start()
            waits.append(copy)
        fetches[name] = waits if whole is None else [pltpu.make_async_copy(whole, whole, sem)]

    def need(*which):
        for name in which:
            for copy in fetches[name]:
                copy.wait()

    fetch("tok", [(hbm["tokens"], tok_v), (hbm["norm_gain"], ng_v)])
    fetch(
        "wqkv",
        [(hbm[w], wqkv_v.at[:, pl.ds(i * hd, hd)]) for i, w in enumerate(("wq", "wk", "wv"))],
    )
    fetch(
        "small",
        [
            (hbm["wf"], wf_v), (hbm["f_bias"], fb_v), (hbm["q_gain"], qg_v),
            (hbm["k_gain"], kg_v), (hbm["gates"], g_v), (hbm["lengths"], len_v),
            (hbm["ffn_gain"], fg_v), (hbm["routes"], rt_v), (hbm["r_weights"], rw_v),
        ],
    )
    fetch("k", [(hbm["keys"].at[s, 0], k_v.at[s]) for s in range(rows)], k_v)

    def fetch_rest():
        fetch(
            "v",
            [
                (hbm["values"].at[s, 0], v_v.at[s // 2, :, pl.ds((s % 2) * hd, hd)])
                for s in range(rows)
            ],
            v_v,
        )
        fetch("wo", [(hbm["wo"], wo_v)])
        gated, downs = [], []
        for k, chip in enumerate(chip_order):
            for half, owner in enumerate((1 - core, core)):
                there = pl.ds(pl.multiple_of((2 * chip + owner) * LANES, LANES), LANES)
                here = pl.ds((half * chips + k) * LANES, LANES)
                after = pl.ds(((1 - half) * chips + k) * LANES, LANES)
                for i in range(2):
                    for n, w in enumerate(("wg", "wu")):
                        cols = pl.ds((2 * i + n) * hidden, hidden)
                        gated.append((hbm[w].at[i, there], wgu_v.at[here, cols]))
                    downs.append(
                        (hbm["wd"].at[i, :, there], wd_v.at[pl.ds(i * hidden, hidden), after])
                    )
        fetch("wgu", gated, wgu_v)
        fetch("wd", downs, wd_v)

    def send(axis, channel, to, src, dst):
        me = lax.axis_index(axis)
        for peer in to:
            pltpu.make_async_remote_copy(
                src_ref=src(peer),
                dst_ref=dst.at[me],
                send_sem=ssem.at[channel],
                recv_sem=rsem.at[channel],
                device_id={axis: peer},
                device_id_type=MESH,
            ).start()

    def wait_all(n, sem, buf):
        part = buf.at[pl.ds(0, n - 1)]
        pltpu.make_async_copy(part, part, sem).wait()

    need("tok")
    normed = norm(tok_v[...].astype(F32), ng_v[...]).astype(BF16)
    for j in range(ep):
        xs[j] = normed[:, j * depth : (j + 1) * depth]
    xr[pl.ds(me_e, 1)] = xs[pl.ds(me_e, 1)]
    pl.semaphore_wait(barrier, ep + tp - 2)
    send("ep", CH_X, peers["ep"], lambda j: xs.at[j], xr)
    fetch_rest()

    need("small")
    row = lax.broadcasted_iota(jnp.int32, (rows, 1), 0)
    diagonal = lax.broadcasted_iota(jnp.int32, (rows, rows), 0) == lax.broadcasted_iota(
        jnp.int32, (rows, rows), 1
    )

    def as_column(line):
        return jnp.sum(jnp.where(diagonal, line, jnp.zeros_like(line)), axis=1, keepdims=True)

    biased = dot_t(normed, wf_v[...]) + fb_v[...]
    own_head = lax.broadcasted_iota(jnp.int32, biased.shape, 1) == me_t
    biased = jnp.sum(jnp.where(own_head, biased, 0.0), axis=1, keepdims=True)
    forget = jnp.minimum(biased, 0.0) - jnp.log1p(jnp.exp(-jnp.abs(biased)))

    lengths = as_column(len_v[...].astype(F32)).astype(jnp.int32)
    position = lax.broadcasted_iota(jnp.int32, (rows, span), 1)
    gates = jnp.zeros((rows, span), F32)
    for s in range(rows):
        gates = jnp.where(row == s, g_v[s], gates)
    last_gate = jnp.sum(jnp.where(position == lengths - 1, gates, 0.0), axis=1, keepdims=True)
    bias = jnp.where(position < lengths, (last_gate - gates) + forget, -1e30)

    first = rt_v[0:1, :]
    second = rt_v[1:2, :]
    slot_col = lax.broadcasted_iota(jnp.int32, (n_slots, rows), 0)
    expert_col, copy_col = lax.div(slot_col, CAP), lax.rem(slot_col, CAP)
    named = ((expert_col == first) | (expert_col == second)).astype(F32)
    before = (
        lax.broadcasted_iota(jnp.int32, (rows, rows), 0)
        < lax.broadcasted_iota(jnp.int32, (rows, rows), 1)
    ).astype(F32)
    earlier = dot(named.astype(BF16), before.astype(BF16))
    placing = jnp.where(earlier == copy_col.astype(F32), named, 0.0).astype(BF16)

    weight_sum = rw_v[0:1, :] + rw_v[1:2, :]
    share_a = as_column(rw_v[0:1, :] / weight_sum)
    share_b = as_column(rw_v[1:2, :] / weight_sum)
    route_a = as_column(first.astype(F32)).astype(jnp.int32)
    route_b = as_column(second.astype(F32)).astype(jnp.int32)
    slot_row = lax.broadcasted_iota(jnp.int32, (rows, n_slots), 1)
    expert_row, copy_row = lax.div(slot_row, CAP), lax.rem(slot_row, CAP)
    is_a, is_b = expert_row == route_a, expert_row == route_b
    after = (
        lax.broadcasted_iota(jnp.int32, (rows, rows), 1)
        < lax.broadcasted_iota(jnp.int32, (rows, rows), 0)
    ).astype(BF16)
    earlier_row = dot(after, (is_a | is_b).astype(F32).astype(BF16))
    combine = jnp.where(is_a, share_a, 0.0) + jnp.where(is_b, share_b, 0.0)
    combine = jnp.where(earlier_row == copy_row.astype(F32), combine, 0.0)
    combine_1 = combine.astype(BF16)
    rest = combine - combine_1.astype(F32)
    combine_2 = rest.astype(BF16)
    combine_3 = (rest - combine_2.astype(F32)).astype(BF16)
    combine_parts = jnp.concatenate([combine_1, combine_2, combine_3], axis=0)

    need("k")
    for s in range(rows):
        kt[s * hd : (s + 1) * hd, :] = k_v[s].T

    need("wqkv")
    wait_all(ep, rsem.at[CH_X], xr)
    part = dot(xr[...].reshape(ep * rows, depth), wqkv_v[...])
    qs[...] = part[:, :hd].reshape(ep, rows, hd)
    send("ep", CH_Q, peers["ep"], lambda j: qs.at[j], qr)
    for j in range(ep):
        own = part[j * rows : (j + 1) * rows]
        kvs[j, 0:rows, :] = own[:, hd : 2 * hd].astype(BF16)
        kvs[j, rows : 2 * rows, :] = own[:, 2 * hd :].astype(BF16)
    send("ep", CH_KV, peers["ep"], lambda j: kvs.at[j], kvr)
    qr[pl.ds(me_e, 1)] = qs[pl.ds(me_e, 1)]
    kvr[pl.ds(me_e, 1)] = kvs[pl.ds(me_e, 1)]
    need("v")
    wait_all(ep, rsem.at[CH_Q], qr)
    queries = norm(jnp.sum(qr[...], axis=0), qg_v[...]).astype(BF16)

    score_scale = hd ** (-0.5)
    wide = queries.astype(F32)
    scores = jnp.zeros((rows, span), F32)
    for pair in range(rows // 2):
        both = [jnp.where(row == 2 * pair + i, wide, 0.0) for i in range(2)]
        both = jnp.concatenate(both, axis=1).astype(BF16)
        scores = scores + dot(both, kt[2 * pair * hd : (2 * pair + 2) * hd, :])
    wait_all(ep, rsem.at[CH_KV], kvr)
    kv_raw = jnp.sum(kvr[...].astype(F32), axis=0)
    keys_new = norm(kv_raw[:rows], kg_v[...]).astype(BF16)
    values_new = kv_raw[rows:].astype(BF16)
    scores = scores * score_scale + bias
    own_score = (
        jnp.sum(queries.astype(F32) * keys_new.astype(F32), axis=1, keepdims=True) * score_scale
    )
    peak = jnp.maximum(jnp.max(scores, axis=1, keepdims=True), own_score)
    weights = jnp.exp(scores - peak)
    own_weight = jnp.exp(own_score - peak)
    denominator = jnp.sum(weights, axis=1, keepdims=True) + own_weight
    probabilities = weights / denominator
    own_prob = (own_weight / denominator).astype(BF16).astype(F32)
    apart = [
        jnp.where(lax.div(row, 2) == pair, probabilities, 0.0).astype(BF16)
        for pair in range(rows // 2)
    ]
    summed = dot(jnp.concatenate(apart, axis=1), v_v[...].reshape(rows // 2 * span, 2 * hd))
    summed = jnp.where(lax.rem(row, 2) == 0, summed[:, :hd], summed[:, hd:])
    attended = (summed + own_prob * values_new.astype(F32)).astype(BF16)

    need("wo")
    cols = or_.shape[2]
    partial = dot(attended, wo_v[...])
    for j in range(tp):
        os_[j] = partial[:, j * cols : (j + 1) * cols].astype(BF16)
    or_[pl.ds(me_t, 1)] = os_[pl.ds(me_t, 1)]
    send("tp", CH_O, peers["tp"], lambda j: os_.at[j], or_)
    wait_all(tp, rsem.at[CH_O], or_)
    own_tokens = tok_v[:, pl.ds(pl.multiple_of(me_t * cols, cols), cols)].astype(F32)
    mixed = (own_tokens + jnp.sum(or_[...].astype(F32), axis=0)).astype(BF16)

    def send_rows(channel, src, dst, recv_sem, step):
        a, b, d = step
        owner = y_at[a] * 4 + x_at[b]
        k = seen_as[d]
        pltpu.make_async_remote_copy(
            src_ref=src(slots * owner),
            dst_ref=dst.at[pl.ds(k * n_slots + slots * me_e, slots)],
            send_sem=ssem.at[channel],
            recv_sem=recv_sem(k),
            device_id={"ep": owner, "tp": z_at[d] * 2 + 1 - core},
            device_id_type=MESH,
        ).start()

    def swap(channel, src, dst, sem, at):
        pltpu.make_async_remote_copy(
            src_ref=src.at[at],
            dst_ref=dst.at[at],
            send_sem=ssem.at[channel],
            recv_sem=sem,
            device_id={"tp": partner},
            device_id_type=MESH,
        ).start()

    def wait_rows(sem, buf):
        pltpu.make_async_copy(buf, buf, sem).wait()

    def block_rows(k, count=1):
        return pl.ds(k * n_slots, count * n_slots)

    ds_[...] = dot(placing, mixed).astype(BF16)
    for step in far_first(outer, 4, chips):
        send_rows(CH_D, lambda at: ds_.at[pl.ds(at, slots)], dr, lambda k: dsem.at[k], step)
    need("wgu", "wd")
    squares = jnp.zeros((n_slots, LANES), F32)
    for k in reversed(range(chips)):
        wait_rows(dsem.at[k], dr.at[block_rows(k)])
        swap(CH_DP, dr, dp, dpsem.at[k], block_rows(k))
        block = dr[block_rows(k), :].astype(F32)
        squares = squares + block * block
    for k in reversed(range(chips)):
        wait_rows(dpsem.at[k], dp.at[block_rows(k)])
        block = dp[block_rows(k), :].astype(F32)
        squares = squares + block * block
    factor = lax.rsqrt(jnp.sum(squares, axis=1, keepdims=True) / width + EPS)
    for half, (buf, owner) in enumerate(((dr, 1 - core), (dp, core))):
        for k, chip in enumerate(chip_order):
            at = pl.multiple_of((2 * chip + owner) * LANES, LANES)
            block = buf[block_rows(k), :].astype(F32) * factor * fg_v[:, pl.ds(at, LANES)]
            here = (half * chips + k) * LANES
            xe[:, here : here + LANES] = block.astype(BF16)

    both = dot(xe[...], wgu_v[...])
    slot_line = lax.broadcasted_iota(jnp.int32, (n_slots, 1), 0)
    kind = lax.div(lax.rem(slot_line, slots), CAP)
    parts = []
    for i in range(2):
        gate = both[:, 2 * i * hidden : (2 * i + 1) * hidden]
        upper = both[:, (2 * i + 1) * hidden : (2 * i + 2) * hidden]
        parts.append(jnp.where(kind == i, gate * jax.nn.sigmoid(gate) * upper, 0.0))
    hidden_rows = jnp.concatenate(parts, axis=1).astype(BF16)

    halves = min(2, chips)
    share = chips // halves
    for half in range(halves):
        first_col = half * share * LANES
        given = dot(hidden_rows, wd_v[:, first_col : first_col + share * LANES]).astype(BF16)
        for n in range(share):
            rg[block_rows(half * share + n), :] = given[:, n * LANES : (n + 1) * LANES]
        swap(CH_RP, rg, rp, rpsem.at[half], block_rows(half * share, share))
    kept = dot(hidden_rows, wd_v[:, chips * LANES :])
    for half in range(halves):
        wait_rows(rpsem.at[half], rp.at[block_rows(half * share, share)])
        for k in range(half * share, (half + 1) * share):
            mine = kept[:, k * LANES : (k + 1) * LANES]
            rs[block_rows(k), :] = (mine + rp[block_rows(k), :].astype(F32)).astype(BF16)
        for a, b, d in far_first(outer, 4, chips):
            k = chip_steps.index(d)
            if k // share == half:
                send_rows(
                    CH_R,
                    lambda at: rs.at[pl.ds(k * n_slots + at, slots)],
                    rr,
                    lambda _: rsem.at[CH_R],
                    (a, b, d),
                )
    wait_rows(rsem.at[CH_R], rr)

    total = jnp.zeros((n_slots, LANES), F32)
    for k in range(chips):
        total = total + rr[block_rows(k), :].astype(F32)
    stacked = dot(combine_parts, total.astype(BF16))
    mix = stacked[:rows] + stacked[rows : 2 * rows] + stacked[2 * rows :]
    out_ref[...] = (mixed.astype(F32) + mix).astype(BF16)

    for channel, n, buf in ((CH_X, ep, xs), (CH_Q, ep, qs), (CH_KV, ep, kvs), (CH_O, tp, os_)):
        wait_all(n, ssem.at[channel], buf)
    for channel, buf in ((CH_D, dr), (CH_DP, dr), (CH_RP, rg), (CH_R, rs)):
        wait_rows(ssem.at[channel], buf)


def local(ep, tp, tokens, norm_gain, w_query, w_key, w_value, w_forget, forget_bias, query_gain,
          key_gain, cache_keys, cache_values, cache_gates, lengths, w_output, ffn_gain, routes,
          route_weights, w_gate, w_up, w_down):
    rows, width = tokens.shape
    span, hd = cache_keys.shape[2], cache_keys.shape[3]
    depth = w_query.shape[0]
    cols = width // tp
    hidden = w_gate.shape[2]
    heads = w_forget.shape[1]
    n_slots = 2 * CAP * ep
    vmem = pltpu.VMEM
    scratch = [
        vmem((rows, width), BF16), vmem((1, width), F32), vmem((depth, 3 * hd), BF16),
        vmem((heads, width), BF16), vmem((1, heads), F32), vmem((1, hd), F32), vmem((1, hd), F32),
        vmem((rows, span, hd), BF16), vmem((rows // 2, span, 2 * hd), BF16), vmem((rows, 1, span), F32),
        vmem((1, rows), jnp.int32), vmem((hd, width), BF16), vmem((1, width), F32),
        vmem((2, rows), jnp.int32), vmem((2, rows), F32), vmem((width, 4 * hidden), BF16),
        vmem((2 * hidden, width), BF16),
        vmem((ep, rows, depth), BF16), vmem((ep, rows, depth), BF16),
        vmem((ep, rows, hd), F32), vmem((ep, rows, hd), F32),
        vmem((ep, 2 * rows, hd), BF16), vmem((ep, 2 * rows, hd), BF16),
        vmem((tp, rows, cols), BF16), vmem((tp, rows, cols), BF16),
        vmem((n_slots, LANES), BF16), *[vmem((tp // 2 * n_slots, LANES), BF16)] * 6,
        vmem((rows * hd, span), BF16), vmem((n_slots, width), BF16),
        pltpu.SemaphoreType.DMA((24,)), pltpu.SemaphoreType.DMA((8,)),
        pltpu.SemaphoreType.DMA((5,)), *[pltpu.SemaphoreType.DMA((tp // 2,))] * 3,
    ]
    operands = (
        tokens, norm_gain[None], w_query, w_key, w_value, w_forget.T, forget_bias[None],
        query_gain[None], key_gain[None], cache_keys, cache_values, cache_gates, lengths[None],
        w_output, ffn_gain[None], routes.T, route_weights.T, w_gate, w_up, w_down,
    )
    return pl.pallas_call(
        functools.partial(kernel, ep, tp),
        out_shape=pltpu.VMEM((rows, cols), BF16),
        in_specs=[pl.BlockSpec(memory_space=pltpu.HBM)] * len(operands),
        out_specs=pl.BlockSpec(memory_space=pltpu.VMEM),
        scratch_shapes=scratch,
        compiler_params=pltpu.CompilerParams(
            collective_id=0, has_side_effects=True, vmem_limit_bytes=67043328 - 65536
        ),
        name="layer",
    )(*operands)


def solution(mesh):
    placed = (
        P("ep", None), P(), P("ep", "tp"), P("ep", "tp"), P("ep", "tp"), P(), P(), P(), P(),
        P("ep", "tp", None, None), P("ep", "tp", None, None), P("ep", "tp", None), P("ep"),
        P("tp", None), P(), P("ep", None), P("ep", None), P("ep", None, "tp"),
        P("ep", None, "tp"), P("ep", "tp", None),
    )
    return jax.shard_map(
        functools.partial(local, mesh.shape["ep"], mesh.shape["tp"]),
        mesh=mesh, in_specs=placed, out_specs=P("ep", "tp"), check_vma=False,
    )
```

```python
import functools
import itertools

import jax
import jax.numpy as jnp
from jax import lax
from jax.experimental import pallas as pl
from jax.experimental.pallas import tpu as pltpu
from jax.sharding import PartitionSpec as P

MESH = pl.DeviceIdType.MESH
F32 = jnp.float32
BF16 = jnp.bfloat16
EPS = 1e-06
CAP = 2
LANES = 128

CH_X, CH_Q, CH_KV, CH_O, CH_R, CH_WQ, CH_WKV, CH_D, CH_DP, CH_RP = range(10)
SHARERS = 8


def norm(v, gain):
    return v * lax.rsqrt(jnp.mean(v * v, axis=-1, keepdims=True) + EPS) * gain


def dot(a, b):
    return jnp.dot(a, b, preferred_element_type=F32)


def dot_t(a, b):
    return lax.dot_general(a, b, (((1,), (1,)), ((), ())), preferred_element_type=F32)


def hops(step, sizes):
    return sum(min(a, n - a) for a, n in zip(step, sizes))


def far_first(*sizes):
    steps = itertools.product(*(range(size) for size in sizes))
    return sorted(steps, key=lambda step: -hops(step, sizes))


def moved(me, size, step):
    return lax.rem(me + step, size) if step else me


def kernel(ep, tp, *refs):
    names = (
        "tokens", "norm_gain", "wq", "wk", "wv", "wf", "f_bias", "q_gain", "k_gain", "keys",
        "values", "gates", "lengths", "wo", "ffn_gain", "routes", "r_weights", "wg", "wu", "wd",
    )
    hbm = dict(zip(names, refs))
    out_ref = refs[len(names)]
    (
        tok_v, ng_v, wq_v, wkv_v, wf_v, fb_v, qg_v, kg_v, k_v, v_v, g_v, len_v,
        wo_v, fg_v, rt_v, rw_v, wgu_v, wd_v,
        xs, xr, qs, qr, kvs, kvr, os_, or_, ds_, dr, dp, rg, rp, rs, rr, kt, xe,
        hsem, ssem, rsem, dsem, dpsem, rpsem,
    ) = refs[len(names) + 1 :]

    me_e, me_t = lax.axis_index("ep"), lax.axis_index("tp")
    rows, width = tok_v.shape
    span, hd = k_v.shape[1], k_v.shape[2]
    depth = xs.shape[2]
    hidden = wd_v.shape[0] // 2
    slots = 2 * CAP
    n_slots = ep * slots

    fetches, taken = {}, itertools.count()

    def fetch(name, pairs, whole=None):
        waits, at = [], next(taken) if whole is not None else None
        for src, dst in pairs:
            sem = hsem.at[next(taken) if whole is None else at]
            copy = pltpu.make_async_copy(src, dst, sem)
            copy.start()
            waits.append(copy)
        fetches[name] = waits if whole is None else [pltpu.make_async_copy(whole, whole, sem)]

    def need(*which):
        for name in which:
            for copy in fetches[name]:
                copy.wait()

    fetch("tok", [(hbm["tokens"], tok_v), (hbm["norm_gain"], ng_v)])

    outer, chips = ep // 4, tp // 2
    y, x = lax.div(me_e, 4), lax.rem(me_e, 4)
    z, core = lax.div(me_t, 2), lax.rem(me_t, 2)
    y_at = [moved(y, outer, a) for a in range(outer)]
    x_at = [moved(x, 4, a) for a in range(4)]
    z_at = [moved(z, chips, a) for a in range(chips)]
    core_at = [core, 1 - core]
    turn = 2 * lax.rem(y, 2)
    y_weights, y_tokens = y + 1 - turn, lax.rem(y + outer - 1 + turn, outer)
    sharers = [(a, x_at[b]) for a, b in far_first(2, 4)[:-1]]
    y_of = (y, y_tokens)
    others = [z_at[a] * 2 + core_at[b] for a, b in far_first(chips, 2)[:-1]]
    partner = z * 2 + 1 - core
    chip_steps = [step for (step,) in far_first(chips)]
    chip_order = [z_at[step] for step in chip_steps]
    seen_as = {step: chip_steps.index(-step % chips) for step in chip_steps}
    barrier = pltpu.get_barrier_semaphore()
    for peer in [y_of[a] * 4 + b for a, b in sharers] + [y_weights * 4 + x]:
        pl.semaphore_signal(barrier, inc=1, device_id={"ep": peer}, device_id_type=MESH)
    for peer in others:
        pl.semaphore_signal(barrier, inc=1, device_id={"tp": peer}, device_id_type=MESH)

    fetch(
        "wqkv",
        [
            (hbm["wq"], wq_v.at[pl.ds(0, depth)]),
            (hbm["wk"], wkv_v.at[pl.ds(0, depth), pl.ds(0, hd)]),
            (hbm["wv"], wkv_v.at[pl.ds(0, depth), pl.ds(hd, hd)]),
        ],
    )
    fetch(
        "small",
        [
            (hbm["wf"], wf_v), (hbm["f_bias"], fb_v), (hbm["q_gain"], qg_v),
            (hbm["k_gain"], kg_v), (hbm["gates"], g_v), (hbm["lengths"], len_v),
            (hbm["ffn_gain"], fg_v), (hbm["routes"], rt_v), (hbm["r_weights"], rw_v),
        ],
    )
    fetch("k", [(hbm["keys"].at[s, 0], k_v.at[s]) for s in range(rows)], k_v)

    def fetch_rest():
        fetch(
            "v",
            [
                (hbm["values"].at[s, 0], v_v.at[s // 2, :, pl.ds((s % 2) * hd, hd)])
                for s in range(rows)
            ],
            v_v,
        )
        fetch("wo", [(hbm["wo"], wo_v)])
        gated, downs = [], []
        for k, chip in enumerate(chip_order):
            for half, owner in enumerate((1 - core, core)):
                there = pl.ds(pl.multiple_of((2 * chip + owner) * LANES, LANES), LANES)
                here = pl.ds((half * chips + k) * LANES, LANES)
                after = pl.ds(((1 - half) * chips + k) * LANES, LANES)
                for i in range(2):
                    for n, w in enumerate(("wg", "wu")):
                        cols = pl.ds((2 * i + n) * hidden, hidden)
                        gated.append((hbm[w].at[i, there], wgu_v.at[here, cols]))
                    downs.append(
                        (hbm["wd"].at[i, :, there], wd_v.at[pl.ds(i * hidden, hidden), after])
                    )
        fetch("wgu", gated, wgu_v)
        fetch("wd", downs, wd_v)

    def send(channel, src, dst, **to):
        pltpu.make_async_remote_copy(
            src_ref=src,
            dst_ref=dst,
            send_sem=ssem.at[channel],
            recv_sem=rsem.at[channel],
            device_id=to,
            device_id_type=MESH,
        ).start()

    def wait_copy(sem, buf):
        pltpu.make_async_copy(buf, buf, sem).wait()

    def wait_all(n, sem, buf):
        part = buf.at[pl.ds(0, n - 1)]
        pltpu.make_async_copy(part, part, sem).wait()

    need("tok")
    normed = norm(tok_v[...].astype(F32), ng_v[...]).astype(BF16)
    for j in range(ep):
        xs[j] = normed[:, j * depth : (j + 1) * depth]
    xr[pl.ds(x, 1)] = xs[pl.ds(me_e, 1)]
    xr[pl.ds(SHARERS + x, 1)] = xs[pl.ds(y_weights * 4 + x, 1)]
    need("wqkv")
    pl.semaphore_wait(barrier, SHARERS + tp - 1)
    own_rows, new_rows = pl.ds(0, depth), pl.ds(depth, depth)
    send(CH_WQ, wq_v.at[own_rows], wq_v.at[new_rows], ep=y_weights * 4 + x)
    blocks_of = ((y, y_weights), (y_tokens, y_tokens + 1 - 2 * lax.rem(y_tokens, 2)))
    for a, b in sharers:
        for n, y_block in enumerate(blocks_of[a]):
            there = xr.at[n * SHARERS + 4 * a + x]
            send(CH_X, xs.at[y_block * 4 + b], there, ep=y_of[a] * 4 + b)
    send(CH_WKV, wkv_v.at[own_rows], wkv_v.at[new_rows], ep=y_weights * 4 + x)
    fetch_rest()

    need("small")
    row = lax.broadcasted_iota(jnp.int32, (rows, 1), 0)
    diagonal = lax.broadcasted_iota(jnp.int32, (rows, rows), 0) == lax.broadcasted_iota(
        jnp.int32, (rows, rows), 1
    )

    def as_column(line):
        return jnp.sum(jnp.where(diagonal, line, jnp.zeros_like(line)), axis=1, keepdims=True)

    biased = dot_t(normed, wf_v[...]) + fb_v[...]
    own_head = lax.broadcasted_iota(jnp.int32, biased.shape, 1) == me_t
    biased = jnp.sum(jnp.where(own_head, biased, 0.0), axis=1, keepdims=True)
    forget = jnp.minimum(biased, 0.0) - jnp.log1p(jnp.exp(-jnp.abs(biased)))

    lengths = as_column(len_v[...].astype(F32)).astype(jnp.int32)
    position = lax.broadcasted_iota(jnp.int32, (rows, span), 1)
    gates = jnp.zeros((rows, span), F32)
    for s in range(rows):
        gates = jnp.where(row == s, g_v[s], gates)
    last_gate = jnp.sum(jnp.where(position == lengths - 1, gates, 0.0), axis=1, keepdims=True)
    bias = jnp.where(position < lengths, (last_gate - gates) + forget, -1e30)

    first = rt_v[0:1, :]
    second = rt_v[1:2, :]
    slot_col = lax.broadcasted_iota(jnp.int32, (n_slots, rows), 0)
    expert_col, copy_col = lax.div(slot_col, CAP), lax.rem(slot_col, CAP)
    named = ((expert_col == first) | (expert_col == second)).astype(F32)
    before = (
        lax.broadcasted_iota(jnp.int32, (rows, rows), 0)
        < lax.broadcasted_iota(jnp.int32, (rows, rows), 1)
    ).astype(F32)
    earlier = dot(named.astype(BF16), before.astype(BF16))
    placing = jnp.where(earlier == copy_col.astype(F32), named, 0.0).astype(BF16)

    weight_sum = rw_v[0:1, :] + rw_v[1:2, :]
    share_a = as_column(rw_v[0:1, :] / weight_sum)
    share_b = as_column(rw_v[1:2, :] / weight_sum)
    route_a = as_column(first.astype(F32)).astype(jnp.int32)
    route_b = as_column(second.astype(F32)).astype(jnp.int32)
    slot_row = lax.broadcasted_iota(jnp.int32, (rows, n_slots), 1)
    expert_row, copy_row = lax.div(slot_row, CAP), lax.rem(slot_row, CAP)
    is_a, is_b = expert_row == route_a, expert_row == route_b
    after = (
        lax.broadcasted_iota(jnp.int32, (rows, rows), 1)
        < lax.broadcasted_iota(jnp.int32, (rows, rows), 0)
    ).astype(BF16)
    earlier_row = dot(after, (is_a | is_b).astype(F32).astype(BF16))
    combine = jnp.where(is_a, share_a, 0.0) + jnp.where(is_b, share_b, 0.0)
    combine = jnp.where(earlier_row == copy_row.astype(F32), combine, 0.0)
    combine_1 = combine.astype(BF16)
    rest = combine - combine_1.astype(F32)
    combine_2 = rest.astype(BF16)
    combine_3 = (rest - combine_2.astype(F32)).astype(BF16)
    combine_parts = jnp.concatenate([combine_1, combine_2, combine_3], axis=0)

    def turn_keys(first_row, last_row):
        for s in range(first_row, last_row):
            kt[s * hd : (s + 1) * hd, :] = k_v[s].T

    need("k")
    turn_keys(0, rows // 2)

    wait_copy(rsem.at[CH_WQ], wq_v.at[new_rows])
    wait_copy(rsem.at[CH_X], xr.at[pl.ds(0, 2 * (SHARERS - 1))])
    inputs = xr[...].reshape(2, SHARERS * rows, depth)
    inputs = jnp.concatenate([inputs[0], inputs[1]], axis=1)
    qs[...] = dot(inputs, wq_v[...]).reshape(SHARERS, rows, hd)
    for a, b in sharers:
        send(CH_Q, qs.at[4 * a + b], qr.at[4 * a + x], ep=y_of[a] * 4 + b)
    turn_keys(rows // 2, rows)
    wait_copy(rsem.at[CH_WKV], wkv_v.at[new_rows])
    part = dot(inputs, wkv_v[...])
    for j in range(SHARERS):
        own = part[j * rows : (j + 1) * rows]
        kvs[j, 0:rows, :] = own[:, :hd].astype(BF16)
        kvs[j, rows : 2 * rows, :] = own[:, hd:].astype(BF16)
    for a, b in sharers:
        send(CH_KV, kvs.at[4 * a + b], kvr.at[4 * a + x], ep=y_of[a] * 4 + b)
    qr[pl.ds(x, 1)] = qs[pl.ds(x, 1)]
    kvr[pl.ds(x, 1)] = kvs[pl.ds(x, 1)]
    need("v")
    wait_all(SHARERS, rsem.at[CH_Q], qr)
    queries = norm(jnp.sum(qr[...], axis=0), qg_v[...]).astype(BF16)

    score_scale = hd ** (-0.5)
    wide = queries.astype(F32)
    scores = jnp.zeros((rows, span), F32)
    for pair in range(rows // 2):
        both = [jnp.where(row == 2 * pair + i, wide, 0.0) for i in range(2)]
        both = jnp.concatenate(both, axis=1).astype(BF16)
        scores = scores + dot(both, kt[2 * pair * hd : (2 * pair + 2) * hd, :])
    wait_all(SHARERS, rsem.at[CH_KV], kvr)
    kv_raw = jnp.sum(kvr[...].astype(F32), axis=0)
    keys_new = norm(kv_raw[:rows], kg_v[...]).astype(BF16)
    values_new = kv_raw[rows:].astype(BF16)
    scores = scores * score_scale + bias
    own_score = (
        jnp.sum(queries.astype(F32) * keys_new.astype(F32), axis=1, keepdims=True) * score_scale
    )
    cached_peak = jnp.max(scores, axis=1, keepdims=True)
    weights = jnp.exp(scores - cached_peak)
    peak = jnp.maximum(cached_peak, own_score)
    lowered = jnp.exp(cached_peak - peak)
    own_weight = jnp.exp(own_score - peak)
    denominator = jnp.sum(weights, axis=1, keepdims=True) * lowered + own_weight
    probabilities = weights * (lowered / denominator)
    own_prob = (own_weight / denominator).astype(BF16).astype(F32)
    apart = [
        jnp.where(lax.div(row, 2) == pair, probabilities, 0.0).astype(BF16)
        for pair in range(rows // 2)
    ]
    summed = dot(jnp.concatenate(apart, axis=1), v_v[...].reshape(rows // 2 * span, 2 * hd))
    summed = jnp.where(lax.rem(row, 2) == 0, summed[:, :hd], summed[:, hd:])
    attended = (summed + own_prob * values_new.astype(F32)).astype(BF16)

    need("wo")
    cols = or_.shape[2]
    partial = dot(attended, wo_v[...])
    for j in range(tp):
        os_[j] = partial[:, j * cols : (j + 1) * cols].astype(BF16)
    or_[pl.ds(me_t, 1)] = os_[pl.ds(me_t, 1)]
    for peer in others:
        send(CH_O, os_.at[peer], or_.at[me_t], tp=peer)
    wait_all(tp, rsem.at[CH_O], or_)
    own_tokens = tok_v[:, pl.ds(pl.multiple_of(me_t * cols, cols), cols)].astype(F32)
    mixed = (own_tokens + jnp.sum(or_[...].astype(F32), axis=0)).astype(BF16)

    def send_rows(channel, src, dst, recv_sem, step):
        a, b, d = step
        owner = y_at[a] * 4 + x_at[b]
        k = seen_as[d]
        pltpu.make_async_remote_copy(
            src_ref=src(slots * owner),
            dst_ref=dst.at[pl.ds(k * n_slots + slots * me_e, slots)],
            send_sem=ssem.at[channel],
            recv_sem=recv_sem(k),
            device_id={"ep": owner, "tp": z_at[d] * 2 + 1 - core},
            device_id_type=MESH,
        ).start()

    def swap(channel, src, dst, sem, at):
        pltpu.make_async_remote_copy(
            src_ref=src.at[at],
            dst_ref=dst.at[at],
            send_sem=ssem.at[channel],
            recv_sem=sem,
            device_id={"tp": partner},
            device_id_type=MESH,
        ).start()

    def block_rows(k, count=1):
        return pl.ds(k * n_slots, count * n_slots)

    ds_[...] = dot(placing, mixed).astype(BF16)
    for step in far_first(outer, 4, chips):
        send_rows(CH_D, lambda at: ds_.at[pl.ds(at, slots)], dr, lambda k: dsem.at[k], step)
    need("wgu", "wd")
    squares = jnp.zeros((n_slots, LANES), F32)
    for k in reversed(range(chips)):
        wait_copy(dsem.at[k], dr.at[block_rows(k)])
        swap(CH_DP, dr, dp, dpsem.at[k], block_rows(k))
        block = dr[block_rows(k), :].astype(F32)
        squares = squares + block * block
    for k in reversed(range(chips)):
        wait_copy(dpsem.at[k], dp.at[block_rows(k)])
        block = dp[block_rows(k), :].astype(F32)
        squares = squares + block * block
    factor = lax.rsqrt(jnp.sum(squares, axis=1, keepdims=True) / width + EPS)
    for half, (buf, owner) in enumerate(((dr, 1 - core), (dp, core))):
        for k, chip in enumerate(chip_order):
            at = pl.multiple_of((2 * chip + owner) * LANES, LANES)
            block = buf[block_rows(k), :].astype(F32) * factor * fg_v[:, pl.ds(at, LANES)]
            here = (half * chips + k) * LANES
            xe[:, here : here + LANES] = block.astype(BF16)

    both = dot(xe[...], wgu_v[...])
    slot_line = lax.broadcasted_iota(jnp.int32, (n_slots, 1), 0)
    kind = lax.div(lax.rem(slot_line, slots), CAP)
    parts = []
    for i in range(2):
        gate = both[:, 2 * i * hidden : (2 * i + 1) * hidden]
        upper = both[:, (2 * i + 1) * hidden : (2 * i + 2) * hidden]
        parts.append(jnp.where(kind == i, gate * jax.nn.sigmoid(gate) * upper, 0.0))
    hidden_rows = jnp.concatenate(parts, axis=1).astype(BF16)

    halves = min(2, chips)
    share = chips // halves
    for half in range(halves):
        first_col = half * share * LANES
        given = dot(hidden_rows, wd_v[:, first_col : first_col + share * LANES]).astype(BF16)
        for n in range(share):
            rg[block_rows(half * share + n), :] = given[:, n * LANES : (n + 1) * LANES]
        swap(CH_RP, rg, rp, rpsem.at[half], block_rows(half * share, share))
    kept = dot(hidden_rows, wd_v[:, chips * LANES :])
    for half in range(halves):
        wait_copy(rpsem.at[half], rp.at[block_rows(half * share, share)])
        for k in range(half * share, (half + 1) * share):
            mine = kept[:, k * LANES : (k + 1) * LANES]
            rs[block_rows(k), :] = (mine + rp[block_rows(k), :].astype(F32)).astype(BF16)
        for a, b, d in far_first(outer, 4, chips):
            k = chip_steps.index(d)
            if k // share == half:
                send_rows(
                    CH_R,
                    lambda at: rs.at[pl.ds(k * n_slots + at, slots)],
                    rr,
                    lambda _: rsem.at[CH_R],
                    (a, b, d),
                )
    wait_copy(rsem.at[CH_R], rr)

    total = jnp.zeros((n_slots, LANES), F32)
    for k in range(chips):
        total = total + rr[block_rows(k), :].astype(F32)
    stacked = dot(combine_parts, total.astype(BF16))
    mix = stacked[:rows] + stacked[rows : 2 * rows] + stacked[2 * rows :]
    out_ref[...] = (mixed.astype(F32) + mix).astype(BF16)

    for channel, n, buf in ((CH_Q, SHARERS, qs), (CH_KV, SHARERS, kvs), (CH_O, tp, os_)):
        wait_all(n, ssem.at[channel], buf)
    wait_copy(ssem.at[CH_X], xr.at[pl.ds(0, 2 * (SHARERS - 1))])
    wait_copy(ssem.at[CH_WQ], wq_v.at[own_rows])
    wait_copy(ssem.at[CH_WKV], wkv_v.at[own_rows])
    for channel, buf in ((CH_D, dr), (CH_DP, dr), (CH_RP, rg), (CH_R, rs)):
        wait_copy(ssem.at[channel], buf)


def local(ep, tp, tokens, norm_gain, w_query, w_key, w_value, w_forget, forget_bias, query_gain,
          key_gain, cache_keys, cache_values, cache_gates, lengths, w_output, ffn_gain, routes,
          route_weights, w_gate, w_up, w_down):
    rows, width = tokens.shape
    span, hd = cache_keys.shape[2], cache_keys.shape[3]
    depth = w_query.shape[0]
    cols = width // tp
    hidden = w_gate.shape[2]
    heads = w_forget.shape[1]
    n_slots = 2 * CAP * ep
    vmem = pltpu.VMEM
    scratch = [
        vmem((rows, width), BF16), vmem((1, width), F32), vmem((2 * depth, hd), BF16),
        vmem((2 * depth, 2 * hd), BF16),
        vmem((heads, width), BF16), vmem((1, heads), F32), vmem((1, hd), F32), vmem((1, hd), F32),
        vmem((rows, span, hd), BF16), vmem((rows // 2, span, 2 * hd), BF16), vmem((rows, 1, span), F32),
        vmem((1, rows), jnp.int32), vmem((hd, width), BF16), vmem((1, width), F32),
        vmem((2, rows), jnp.int32), vmem((2, rows), F32), vmem((width, 4 * hidden), BF16),
        vmem((2 * hidden, width), BF16),
        vmem((ep, rows, depth), BF16), vmem((2 * SHARERS, rows, depth), BF16),
        vmem((SHARERS, rows, hd), F32), vmem((SHARERS, rows, hd), F32),
        vmem((SHARERS, 2 * rows, hd), BF16), vmem((SHARERS, 2 * rows, hd), BF16),
        vmem((tp, rows, cols), BF16), vmem((tp, rows, cols), BF16),
        vmem((n_slots, LANES), BF16), *[vmem((tp // 2 * n_slots, LANES), BF16)] * 6,
        vmem((rows * hd, span), BF16), vmem((n_slots, width), BF16),
        pltpu.SemaphoreType.DMA((24,)), pltpu.SemaphoreType.DMA((10,)),
        pltpu.SemaphoreType.DMA((7,)), *[pltpu.SemaphoreType.DMA((tp // 2,))] * 3,
    ]
    operands = (
        tokens, norm_gain[None], w_query, w_key, w_value, w_forget.T, forget_bias[None],
        query_gain[None], key_gain[None], cache_keys, cache_values, cache_gates, lengths[None],
        w_output, ffn_gain[None], routes.T, route_weights.T, w_gate, w_up, w_down,
    )
    return pl.pallas_call(
        functools.partial(kernel, ep, tp),
        out_shape=pltpu.VMEM((rows, cols), BF16),
        in_specs=[pl.BlockSpec(memory_space=pltpu.HBM)] * len(operands),
        out_specs=pl.BlockSpec(memory_space=pltpu.VMEM),
        scratch_shapes=scratch,
        compiler_params=pltpu.CompilerParams(
            collective_id=0, has_side_effects=True, vmem_limit_bytes=67043328 - 65536
        ),
        name="layer",
    )(*operands)


def solution(mesh):
    placed = (
        P("ep", None), P(), P("ep", "tp"), P("ep", "tp"), P("ep", "tp"), P(), P(), P(), P(),
        P("ep", "tp", None, None), P("ep", "tp", None, None), P("ep", "tp", None), P("ep"),
        P("tp", None), P(), P("ep", None), P("ep", None), P("ep", None, "tp"),
        P("ep", None, "tp"), P("ep", "tp", None),
    )
    return jax.shard_map(
        functools.partial(local, mesh.shape["ep"], mesh.shape["tp"]),
        mesh=mesh, in_specs=placed, out_specs=P("ep", "tp"), check_vma=False,
    )
```

```python
import functools
import itertools

import jax
import jax.numpy as jnp
from jax import lax
from jax.experimental import pallas as pl
from jax.experimental.pallas import tpu as pltpu
from jax.sharding import PartitionSpec as P

MESH = pl.DeviceIdType.MESH
F32 = jnp.float32
BF16 = jnp.bfloat16
EPS = 1e-06
CAP = 2
LANES = 128

CH_X, CH_Q, CH_KV, CH_O, CH_R, CH_WQ, CH_WKV, CH_D, CH_DP, CH_RP = range(10)
SHARERS = 8


def norm(v, gain):
    return v * lax.rsqrt(jnp.mean(v * v, axis=-1, keepdims=True) + EPS) * gain


def dot(a, b):
    return jnp.dot(a, b, preferred_element_type=F32)


def dot_t(a, b):
    return lax.dot_general(a, b, (((1,), (1,)), ((), ())), preferred_element_type=F32)


def hops(step, sizes):
    return sum(min(a, n - a) for a, n in zip(step, sizes))


def far_first(*sizes):
    steps = itertools.product(*(range(size) for size in sizes))
    return sorted(steps, key=lambda step: -hops(step, sizes))


def moved(me, size, step):
    return lax.rem(me + step, size) if step else me


def kernel(ep, tp, *refs):
    names = (
        "tokens", "norm_gain", "wq", "wk", "wv", "wf", "f_bias", "q_gain", "k_gain", "keys",
        "values", "gates", "lengths", "wo", "ffn_gain", "routes", "r_weights", "wg", "wu", "wd",
    )
    hbm = dict(zip(names, refs))
    out_ref = refs[len(names)]
    (
        tok_v, ng_v, wq_v, wkv_v, wf_v, fb_v, qg_v, kg_v, k_v, v_v, g_v, len_v,
        wo_v, fg_v, rt_v, rw_v, wgu_v, wd_v,
        xs, xr, qs, qr, kvs, kvr, os_, or_, ds_, dr, dp, rg, rp, rs, rr, kt, xe,
        hsem, ssem, rsem, dsem, dpsem, rpsem,
    ) = refs[len(names) + 1 :]

    me_e, me_t = lax.axis_index("ep"), lax.axis_index("tp")
    rows, width = tok_v.shape
    span, hd = k_v.shape[1], k_v.shape[2]
    depth = xs.shape[2]
    hidden = wd_v.shape[0] // 2
    slots = 2 * CAP
    n_slots = ep * slots

    fetches, taken = {}, itertools.count()

    def fetch(name, pairs, whole=None):
        waits, at = [], next(taken) if whole is not None else None
        for src, dst in pairs:
            sem = hsem.at[next(taken) if whole is None else at]
            copy = pltpu.make_async_copy(src, dst, sem)
            copy.start()
            waits.append(copy)
        fetches[name] = waits if whole is None else [pltpu.make_async_copy(whole, whole, sem)]

    def need(*which):
        for name in which:
            for copy in fetches[name]:
                copy.wait()

    fetch("tok", [(hbm["tokens"], tok_v), (hbm["norm_gain"], ng_v)])

    outer, chips = ep // 4, tp // 2
    y, x = lax.div(me_e, 4), lax.rem(me_e, 4)
    z, core = lax.div(me_t, 2), lax.rem(me_t, 2)
    y_at = [moved(y, outer, a) for a in range(outer)]
    x_at = [moved(x, 4, a) for a in range(4)]
    z_at = [moved(z, chips, a) for a in range(chips)]
    core_at = [core, 1 - core]
    turn = 2 * lax.rem(y, 2)
    y_weights, y_tokens = y + 1 - turn, lax.rem(y + outer - 1 + turn, outer)
    sharers = [(a, x_at[b]) for a, b in far_first(2, 4)[:-1]]
    y_of = (y, y_tokens)
    others = [z_at[a] * 2 + core_at[b] for a, b in far_first(chips, 2)[:-1]]
    partner = z * 2 + 1 - core
    chip_steps = [step for (step,) in far_first(chips)]
    chip_order = [z_at[step] for step in chip_steps]
    seen_as = {step: chip_steps.index(-step % chips) for step in chip_steps}
    barrier = pltpu.get_barrier_semaphore()
    for peer in [y_of[a] * 4 + b for a, b in sharers] + [y_weights * 4 + x]:
        pl.semaphore_signal(barrier, inc=1, device_id={"ep": peer}, device_id_type=MESH)
    for peer in others:
        pl.semaphore_signal(barrier, inc=1, device_id={"tp": peer}, device_id_type=MESH)

    fetch(
        "wqkv",
        [
            (hbm["wq"], wq_v.at[pl.ds(0, depth)]),
            (hbm["wk"], wkv_v.at[pl.ds(0, depth), pl.ds(0, hd)]),
            (hbm["wv"], wkv_v.at[pl.ds(0, depth), pl.ds(hd, hd)]),
        ],
    )
    fetch(
        "small",
        [
            (hbm["wf"], wf_v), (hbm["f_bias"], fb_v), (hbm["q_gain"], qg_v),
            (hbm["k_gain"], kg_v), (hbm["gates"], g_v), (hbm["lengths"], len_v),
            (hbm["ffn_gain"], fg_v), (hbm["routes"], rt_v), (hbm["r_weights"], rw_v),
        ],
    )
    fetch("k", [(hbm["keys"].at[s, 0], k_v.at[s]) for s in range(rows)], k_v)

    def fetch_rest():
        fetch(
            "v",
            [
                (hbm["values"].at[s, 0], v_v.at[s // 2, :, pl.ds((s % 2) * hd, hd)])
                for s in range(rows)
            ],
            v_v,
        )
        fetch("wo", [(hbm["wo"], wo_v)])
        gated, downs = [], []
        for k, chip in enumerate(chip_order):
            for half, owner in enumerate((1 - core, core)):
                there = pl.ds(pl.multiple_of((2 * chip + owner) * LANES, LANES), LANES)
                here = pl.ds((half * chips + k) * LANES, LANES)
                after = pl.ds(((1 - half) * chips + k) * LANES, LANES)
                for i in range(2):
                    for n, w in enumerate(("wg", "wu")):
                        cols = pl.ds((2 * i + n) * hidden, hidden)
                        gated.append((hbm[w].at[i, there], wgu_v.at[here, cols]))
                    downs.append(
                        (hbm["wd"].at[i, :, there], wd_v.at[pl.ds(i * hidden, hidden), after])
                    )
        fetch("wgu", gated, wgu_v)
        fetch("wd", downs, wd_v)

    def send(channel, src, dst, **to):
        pltpu.make_async_remote_copy(
            src_ref=src,
            dst_ref=dst,
            send_sem=ssem.at[channel],
            recv_sem=rsem.at[channel],
            device_id=to,
            device_id_type=MESH,
        ).start()

    def wait_copy(sem, buf):
        pltpu.make_async_copy(buf, buf, sem).wait()

    def wait_all(n, sem, buf):
        part = buf.at[pl.ds(0, n - 1)]
        pltpu.make_async_copy(part, part, sem).wait()

    need("tok")
    normed = norm(tok_v[...].astype(F32), ng_v[...]).astype(BF16)
    for j in range(ep):
        xs[j] = normed[:, j * depth : (j + 1) * depth]
    xr[pl.ds(x, 1)] = xs[pl.ds(me_e, 1)]
    xr[pl.ds(SHARERS + x, 1)] = xs[pl.ds(y_weights * 4 + x, 1)]
    need("wqkv")
    pl.semaphore_wait(barrier, SHARERS + tp - 1)
    own_rows, new_rows = pl.ds(0, depth), pl.ds(depth, depth)
    send(CH_WQ, wq_v.at[own_rows], wq_v.at[new_rows], ep=y_weights * 4 + x)
    blocks_of = ((y, y_weights), (y_tokens, y_tokens + 1 - 2 * lax.rem(y_tokens, 2)))
    for a, b in sharers:
        for n, y_block in enumerate(blocks_of[a]):
            there = xr.at[n * SHARERS + 4 * a + x]
            send(CH_X, xs.at[y_block * 4 + b], there, ep=y_of[a] * 4 + b)
    send(CH_WKV, wkv_v.at[own_rows], wkv_v.at[new_rows], ep=y_weights * 4 + x)
    fetch_rest()

    need("small")
    row = lax.broadcasted_iota(jnp.int32, (rows, 1), 0)
    diagonal = lax.broadcasted_iota(jnp.int32, (rows, rows), 0) == lax.broadcasted_iota(
        jnp.int32, (rows, rows), 1
    )

    def as_column(line):
        return jnp.sum(jnp.where(diagonal, line, jnp.zeros_like(line)), axis=1, keepdims=True)

    biased = dot_t(normed, wf_v[...]) + fb_v[...]
    own_head = lax.broadcasted_iota(jnp.int32, biased.shape, 1) == me_t
    biased = jnp.sum(jnp.where(own_head, biased, 0.0), axis=1, keepdims=True)
    forget = jnp.minimum(biased, 0.0) - jnp.log1p(jnp.exp(-jnp.abs(biased)))

    lengths = as_column(len_v[...].astype(F32)).astype(jnp.int32)
    position = lax.broadcasted_iota(jnp.int32, (rows, span), 1)
    gates = jnp.zeros((rows, span), F32)
    for s in range(rows):
        gates = jnp.where(row == s, g_v[s], gates)
    last_gate = jnp.sum(jnp.where(position == lengths - 1, gates, 0.0), axis=1, keepdims=True)
    bias = jnp.where(position < lengths, (last_gate - gates) + forget, -1e30)

    first = rt_v[0:1, :]
    second = rt_v[1:2, :]
    slot_col = lax.broadcasted_iota(jnp.int32, (n_slots, rows), 0)
    expert_col, copy_col = lax.div(slot_col, CAP), lax.rem(slot_col, CAP)
    named = ((expert_col == first) | (expert_col == second)).astype(F32)
    before = (
        lax.broadcasted_iota(jnp.int32, (rows, rows), 0)
        < lax.broadcasted_iota(jnp.int32, (rows, rows), 1)
    ).astype(F32)
    earlier = dot(named.astype(BF16), before.astype(BF16))
    placing = jnp.where(earlier == copy_col.astype(F32), named, 0.0).astype(BF16)

    weight_sum = rw_v[0:1, :] + rw_v[1:2, :]
    share_a = as_column(rw_v[0:1, :] / weight_sum)
    share_b = as_column(rw_v[1:2, :] / weight_sum)
    route_a = as_column(first.astype(F32)).astype(jnp.int32)
    route_b = as_column(second.astype(F32)).astype(jnp.int32)
    slot_row = lax.broadcasted_iota(jnp.int32, (rows, n_slots), 1)
    expert_row, copy_row = lax.div(slot_row, CAP), lax.rem(slot_row, CAP)
    is_a, is_b = expert_row == route_a, expert_row == route_b
    after = (
        lax.broadcasted_iota(jnp.int32, (rows, rows), 1)
        < lax.broadcasted_iota(jnp.int32, (rows, rows), 0)
    ).astype(BF16)
    earlier_row = dot(after, (is_a | is_b).astype(F32).astype(BF16))
    combine = jnp.where(is_a, share_a, 0.0) + jnp.where(is_b, share_b, 0.0)
    combine = jnp.where(earlier_row == copy_row.astype(F32), combine, 0.0)
    combine_1 = combine.astype(BF16)
    rest = combine - combine_1.astype(F32)
    combine_2 = rest.astype(BF16)
    combine_3 = (rest - combine_2.astype(F32)).astype(BF16)
    combine_parts = jnp.concatenate([combine_1, combine_2, combine_3], axis=0)

    def turn_keys(first_row, last_row):
        for s in range(first_row, last_row):
            kt[s * hd : (s + 1) * hd, :] = k_v[s].T

    need("k")
    turn_keys(0, rows // 2)

    wait_copy(rsem.at[CH_WQ], wq_v.at[new_rows])
    wait_copy(rsem.at[CH_X], xr.at[pl.ds(0, 2 * (SHARERS - 1))])
    inputs = xr[...].reshape(2, SHARERS * rows, depth)
    inputs = jnp.concatenate([inputs[0], inputs[1]], axis=1)
    qs[...] = dot(inputs, wq_v[...]).reshape(SHARERS, rows, hd)
    for a, b in sharers:
        send(CH_Q, qs.at[4 * a + b], qr.at[4 * a + x], ep=y_of[a] * 4 + b)
    turn_keys(rows // 2, rows)
    wait_copy(rsem.at[CH_WKV], wkv_v.at[new_rows])
    part = dot(inputs, wkv_v[...])
    for j in range(SHARERS):
        own = part[j * rows : (j + 1) * rows]
        kvs[j, 0:rows, :] = own[:, :hd].astype(BF16)
        kvs[j, rows : 2 * rows, :] = own[:, hd:].astype(BF16)
    for a, b in sharers:
        send(CH_KV, kvs.at[4 * a + b], kvr.at[4 * a + x], ep=y_of[a] * 4 + b)
    qr[pl.ds(x, 1)] = qs[pl.ds(x, 1)]
    kvr[pl.ds(x, 1)] = kvs[pl.ds(x, 1)]
    need("v")
    wait_all(SHARERS, rsem.at[CH_Q], qr)
    queries = norm(jnp.sum(qr[...], axis=0), qg_v[...]).astype(BF16)

    score_scale = hd ** (-0.5)
    wide = queries.astype(F32)
    scores = jnp.zeros((rows, span), F32)
    for pair in range(rows // 2):
        both = [jnp.where(row == 2 * pair + i, wide, 0.0) for i in range(2)]
        both = jnp.concatenate(both, axis=1).astype(BF16)
        scores = scores + dot(both, kt[2 * pair * hd : (2 * pair + 2) * hd, :])
    wait_all(SHARERS, rsem.at[CH_KV], kvr)
    kv_raw = jnp.sum(kvr[...].astype(F32), axis=0)
    keys_new = norm(kv_raw[:rows], kg_v[...]).astype(BF16)
    values_new = kv_raw[rows:].astype(BF16)
    scores = scores * score_scale + bias
    own_score = (
        jnp.sum(queries.astype(F32) * keys_new.astype(F32), axis=1, keepdims=True) * score_scale
    )
    cached_peak = jnp.max(scores, axis=1, keepdims=True)
    weights = jnp.exp(scores - cached_peak)
    peak = jnp.maximum(cached_peak, own_score)
    lowered = jnp.exp(cached_peak - peak)
    own_weight = jnp.exp(own_score - peak)
    denominator = jnp.sum(weights, axis=1, keepdims=True) * lowered + own_weight
    own_prob = (own_weight / denominator).astype(BF16).astype(F32)
    apart = [
        jnp.where(lax.div(row, 2) == pair, weights, 0.0).astype(BF16) for pair in range(rows // 2)
    ]
    summed = dot(jnp.concatenate(apart, axis=1), v_v[...].reshape(rows // 2 * span, 2 * hd))
    summed = jnp.where(lax.rem(row, 2) == 0, summed[:, :hd], summed[:, hd:])
    summed = summed * (lowered / denominator)
    attended = (summed + own_prob * values_new.astype(F32)).astype(BF16)

    need("wo")
    cols = or_.shape[2]
    partial = dot(attended, wo_v[...])
    for j in range(tp):
        os_[j] = partial[:, j * cols : (j + 1) * cols].astype(BF16)
    or_[pl.ds(me_t, 1)] = os_[pl.ds(me_t, 1)]
    for peer in others:
        send(CH_O, os_.at[peer], or_.at[me_t], tp=peer)
    wait_all(tp, rsem.at[CH_O], or_)
    own_tokens = tok_v[:, pl.ds(pl.multiple_of(me_t * cols, cols), cols)].astype(F32)
    mixed = (own_tokens + jnp.sum(or_[...].astype(F32), axis=0)).astype(BF16)

    def send_rows(channel, src, dst, recv_sem, step):
        a, b, d = step
        owner = y_at[a] * 4 + x_at[b]
        k = seen_as[d]
        pltpu.make_async_remote_copy(
            src_ref=src(slots * owner),
            dst_ref=dst.at[pl.ds(k * n_slots + slots * me_e, slots)],
            send_sem=ssem.at[channel],
            recv_sem=recv_sem(k),
            device_id={"ep": owner, "tp": z_at[d] * 2 + 1 - core},
            device_id_type=MESH,
        ).start()

    def swap(channel, src, dst, sem, at):
        pltpu.make_async_remote_copy(
            src_ref=src.at[at],
            dst_ref=dst.at[at],
            send_sem=ssem.at[channel],
            recv_sem=sem,
            device_id={"tp": partner},
            device_id_type=MESH,
        ).start()

    def block_rows(k, count=1):
        return pl.ds(k * n_slots, count * n_slots)

    ds_[...] = dot(placing, mixed).astype(BF16)
    for step in far_first(outer, 4, chips):
        send_rows(CH_D, lambda at: ds_.at[pl.ds(at, slots)], dr, lambda k: dsem.at[k], step)
    need("wgu", "wd")
    squares = jnp.zeros((n_slots, LANES), F32)
    for k in reversed(range(chips)):
        wait_copy(dsem.at[k], dr.at[block_rows(k)])
        swap(CH_DP, dr, dp, dpsem.at[k], block_rows(k))
        block = dr[block_rows(k), :].astype(F32)
        squares = squares + block * block
    for k in reversed(range(chips)):
        wait_copy(dpsem.at[k], dp.at[block_rows(k)])
        block = dp[block_rows(k), :].astype(F32)
        squares = squares + block * block
    factor = lax.rsqrt(jnp.sum(squares, axis=1, keepdims=True) / width + EPS)
    for half, (buf, owner) in enumerate(((dr, 1 - core), (dp, core))):
        for k, chip in enumerate(chip_order):
            at = pl.multiple_of((2 * chip + owner) * LANES, LANES)
            block = buf[block_rows(k), :].astype(F32) * factor * fg_v[:, pl.ds(at, LANES)]
            here = (half * chips + k) * LANES
            xe[:, here : here + LANES] = block.astype(BF16)

    both = dot(xe[...], wgu_v[...])
    slot_line = lax.broadcasted_iota(jnp.int32, (n_slots, 1), 0)
    kind = lax.div(lax.rem(slot_line, slots), CAP)
    parts = []
    for i in range(2):
        gate = both[:, 2 * i * hidden : (2 * i + 1) * hidden]
        upper = both[:, (2 * i + 1) * hidden : (2 * i + 2) * hidden]
        parts.append(jnp.where(kind == i, gate * jax.nn.sigmoid(gate) * upper, 0.0))
    hidden_rows = jnp.concatenate(parts, axis=1).astype(BF16)

    halves = min(2, chips)
    share = chips // halves
    for half in range(halves):
        first_col = half * share * LANES
        given = dot(hidden_rows, wd_v[:, first_col : first_col + share * LANES]).astype(BF16)
        for n in range(share):
            rg[block_rows(half * share + n), :] = given[:, n * LANES : (n + 1) * LANES]
        swap(CH_RP, rg, rp, rpsem.at[half], block_rows(half * share, share))
    kept = dot(hidden_rows, wd_v[:, chips * LANES :])
    for half in range(halves):
        wait_copy(rpsem.at[half], rp.at[block_rows(half * share, share)])
        for k in range(half * share, (half + 1) * share):
            mine = kept[:, k * LANES : (k + 1) * LANES]
            rs[block_rows(k), :] = (mine + rp[block_rows(k), :].astype(F32)).astype(BF16)
        for a, b, d in far_first(outer, 4, chips):
            k = chip_steps.index(d)
            if k // share == half:
                send_rows(
                    CH_R,
                    lambda at: rs.at[pl.ds(k * n_slots + at, slots)],
                    rr,
                    lambda _: rsem.at[CH_R],
                    (a, b, d),
                )
    wait_copy(rsem.at[CH_R], rr)

    total = jnp.zeros((n_slots, LANES), F32)
    for k in range(chips):
        total = total + rr[block_rows(k), :].astype(F32)
    stacked = dot(combine_parts, total.astype(BF16))
    mix = stacked[:rows] + stacked[rows : 2 * rows] + stacked[2 * rows :]
    out_ref[...] = (mixed.astype(F32) + mix).astype(BF16)

    for channel, n, buf in ((CH_Q, SHARERS, qs), (CH_KV, SHARERS, kvs), (CH_O, tp, os_)):
        wait_all(n, ssem.at[channel], buf)
    wait_copy(ssem.at[CH_X], xr.at[pl.ds(0, 2 * (SHARERS - 1))])
    wait_copy(ssem.at[CH_WQ], wq_v.at[own_rows])
    wait_copy(ssem.at[CH_WKV], wkv_v.at[own_rows])
    for channel, buf in ((CH_D, dr), (CH_DP, dr), (CH_RP, rg), (CH_R, rs)):
        wait_copy(ssem.at[channel], buf)


def local(ep, tp, tokens, norm_gain, w_query, w_key, w_value, w_forget, forget_bias, query_gain,
          key_gain, cache_keys, cache_values, cache_gates, lengths, w_output, ffn_gain, routes,
          route_weights, w_gate, w_up, w_down):
    rows, width = tokens.shape
    span, hd = cache_keys.shape[2], cache_keys.shape[3]
    depth = w_query.shape[0]
    cols = width // tp
    hidden = w_gate.shape[2]
    heads = w_forget.shape[1]
    n_slots = 2 * CAP * ep
    vmem = pltpu.VMEM
    scratch = [
        vmem((rows, width), BF16), vmem((1, width), F32), vmem((2 * depth, hd), BF16),
        vmem((2 * depth, 2 * hd), BF16),
        vmem((heads, width), BF16), vmem((1, heads), F32), vmem((1, hd), F32), vmem((1, hd), F32),
        vmem((rows, span, hd), BF16), vmem((rows // 2, span, 2 * hd), BF16), vmem((rows, 1, span), F32),
        vmem((1, rows), jnp.int32), vmem((hd, width), BF16), vmem((1, width), F32),
        vmem((2, rows), jnp.int32), vmem((2, rows), F32), vmem((width, 4 * hidden), BF16),
        vmem((2 * hidden, width), BF16),
        vmem((ep, rows, depth), BF16), vmem((2 * SHARERS, rows, depth), BF16),
        vmem((SHARERS, rows, hd), F32), vmem((SHARERS, rows, hd), F32),
        vmem((SHARERS, 2 * rows, hd), BF16), vmem((SHARERS, 2 * rows, hd), BF16),
        vmem((tp, rows, cols), BF16), vmem((tp, rows, cols), BF16),
        vmem((n_slots, LANES), BF16), *[vmem((tp // 2 * n_slots, LANES), BF16)] * 6,
        vmem((rows * hd, span), BF16), vmem((n_slots, width), BF16),
        pltpu.SemaphoreType.DMA((24,)), pltpu.SemaphoreType.DMA((10,)),
        pltpu.SemaphoreType.DMA((7,)), *[pltpu.SemaphoreType.DMA((tp // 2,))] * 3,
    ]
    operands = (
        tokens, norm_gain[None], w_query, w_key, w_value, w_forget.T, forget_bias[None],
        query_gain[None], key_gain[None], cache_keys, cache_values, cache_gates, lengths[None],
        w_output, ffn_gain[None], routes.T, route_weights.T, w_gate, w_up, w_down,
    )
    return pl.pallas_call(
        functools.partial(kernel, ep, tp),
        out_shape=pltpu.VMEM((rows, cols), BF16),
        in_specs=[pl.BlockSpec(memory_space=pltpu.HBM)] * len(operands),
        out_specs=pl.BlockSpec(memory_space=pltpu.VMEM),
        scratch_shapes=scratch,
        compiler_params=pltpu.CompilerParams(
            collective_id=0, has_side_effects=True, vmem_limit_bytes=67043328 - 65536
        ),
        name="layer",
    )(*operands)


def solution(mesh):
    placed = (
        P("ep", None), P(), P("ep", "tp"), P("ep", "tp"), P("ep", "tp"), P(), P(), P(), P(),
        P("ep", "tp", None, None), P("ep", "tp", None, None), P("ep", "tp", None), P("ep"),
        P("tp", None), P(), P("ep", None), P("ep", None), P("ep", None, "tp"),
        P("ep", None, "tp"), P("ep", "tp", None),
    )
    return jax.shard_map(
        functools.partial(local, mesh.shape["ep"], mesh.shape["tp"]),
        mesh=mesh, in_specs=placed, out_specs=P("ep", "tp"), check_vma=False,
    )
```
